32 devices in a mesh: sp: 8 (over z, y), tp: 4 (over x, core).
Axes of the slice: x: 2, y: 2, z: 4, core: 2. Of those that a mesh axis runs over, the one named last changes fastest.
Arguments:
- mixer_input: bfloat16 [1024, 1024], P('sp', 'tp'), may hold values from -1800 to 1800
- time_step: float32 [2, 64], P(None, 'tp'), may hold values from 0 to 2, as said below
- damping: float32 [2, 1024, 64], P(None, 'sp', 'tp'), may hold values from 0 to 2
- input_map: bfloat16 [2, 2, 64, 64, 16], P(None, None, 'tp'), may hold values from -1 to 1
- readout: float32 [2, 2, 64, 16, 64], P(None, None, 'tp'), may hold values from -0.5 to 0.5
- skip_gain: float32 [1024], P('tp'), may hold values from -4 to 4
- out_gain: float32 [1024], P('tp'), may hold values from 0.1 to 1.9
- out_weight: bfloat16 [1024, 2048], replicated, may hold values from -0.1875 to 0.1875
- residual: bfloat16 [1024, 2048], P(('sp', 'tp')), may hold values from -6 to 6
- channel_gain: float32 [2048], replicated, may hold values from 0.1 to 1.9
- value_weight: bfloat16 [2048, 6144], P('sp', 'tp'), may hold values from -0.125 to 0.125
- gate_weight: bfloat16 [2048, 6144], P('sp', 'tp'), may hold values from -0.125 to 0.125
- value_taps: float32 [3, 6144], P(None, 'tp'), may hold values from -3 to 3
- gate_taps: float32 [3, 6144], P(None, 'tp'), may hold values from -3 to 3
- down_weight: bfloat16 [6144, 2048], P('tp', 'sp'), may hold values from -0.078125 to 0.078125
Outputs:
- output: bfloat16 [1024, 2048], P(('sp', 'tp'))
The draws below stay inside these ranges and needn't reach their ends.
Inputs may be any that keep to these rules, and one draw needn't show every extreme that they name: `time_step`: positive.
All inputs are finite; a program needn't handle non-finite values.
Results may differ from the reference program's by a relative error of at most 0.017.
Values may be sent and summed in bfloat16 or wider, within the bound.
No kernel may reach another device: no remote copies, remote signals or barrier semaphores. Data moves between devices by JAX's collectives and lax.ppermute only.
A program may use at most 128 MiB of HBM per device.

```python
import math
import jax
import jax.numpy as jnp
from jax import lax

D = 2048
DS = 1024
GROUP = 16
STATE = 64
FF = 6144
TOK_DEV = 128
G = 64
TOKEN_POSITIONS = 1024
N_TP = 4


def draw_mixer_input(key, part):
    split_random_keys = jax.random.split(key, 3)
    column_pos = jnp.arange(DS, dtype=jnp.float32) / DS
    spread = math.log(10.0)
    noise = jnp.clip(jax.random.normal(split_random_keys[0], (TOKEN_POSITIONS, DS), jnp.float32), -5.0, 5.0)
    row_scale = jnp.exp(jax.random.uniform(split_random_keys[2], (TOKEN_POSITIONS, 1), jnp.float32, 0.0, spread))
    column_scale = jnp.exp(spread * column_pos)[None, :]
    return (noise * row_scale * column_scale).astype(jnp.float32).astype(jnp.bfloat16)


def draw_time_step(key, part):
    split_random_keys = jax.random.split(key, 3)
    group_count = DS // GROUP
    chance = jax.random.randint(split_random_keys[0], (2, group_count), 0, 16)
    quick = chance < 8
    quick_rate = jnp.exp(jax.random.uniform(split_random_keys[1], (2, group_count), jnp.float32, math.log(5.0 / TOK_DEV), math.log(16.0 / TOK_DEV)))
    slow_rate = jnp.exp(jax.random.uniform(split_random_keys[2], (2, group_count), jnp.float32, math.log(0.2 / TOKEN_POSITIONS), math.log(1.0 / TOKEN_POSITIONS)))
    return 2.0 * jnp.where(quick, quick_rate, slow_rate)


def draw_damping(key, part):
    split_random_keys = jax.random.split(key, 4)
    group_count = DS // GROUP
    blocks = TOKEN_POSITIONS // TOK_DEV
    baseline_rate = jnp.exp(jax.random.uniform(split_random_keys[0], (2, 1, group_count), jnp.float32, math.log(0.1), math.log(0.4))) / TOKEN_POSITIONS
    multiplier = jnp.exp(jax.random.uniform(split_random_keys[1], (2, blocks, group_count), jnp.float32, 0.0, math.log(4.0)))
    multiplier = jnp.repeat(multiplier, TOK_DEV, axis=1)
    spike_locations = jax.random.randint(split_random_keys[2], (2, 1, group_count, 3), 0, TOKEN_POSITIONS)
    dropped_fraction = jax.random.uniform(split_random_keys[3], (2, 1, group_count, 3), jnp.float32, 0.2, 0.33)
    token_position = jnp.arange(TOKEN_POSITIONS, dtype=jnp.int32)[None, :, None, None]
    sudden_spike = jnp.sum(jnp.where(token_position == spike_locations, -jnp.log1p(-dropped_fraction), 0.0), axis=3)
    return (baseline_rate * multiplier + sudden_spike).astype(jnp.float32)


def block_levels(rng, dims, cuts, smallest, top_value):
    level, own = 1.0, jax.random.fold_in(rng, 6)
    for axis_at, shards_of in cuts:
        draws = jnp.exp(jax.random.uniform(jax.random.fold_in(own, axis_at), (shards_of,), jnp.float32, smallest / len(cuts), top_value / len(cuts)))
        level = level * jnp.repeat(draws, dims[axis_at] // shards_of).reshape([-1 if axis == axis_at else 1 for axis in range(len(dims))])
    return level


def normal_values(rng, extent, scale, limit, cuts=(), kind=jnp.bfloat16):
    level = block_levels(rng, extent, cuts, -0.22, 0.18) if cuts else 1.0
    array = jax.random.normal(rng, extent, jnp.float32) * scale * level
    return jnp.minimum(jnp.maximum(array, -limit), limit).astype(kind)


def setup_inputs(seed: int = 0) -> dict:
    key_of = jax.random.split(jax.random.key(seed), 16)
    mixer_input = draw_mixer_input(jax.random.fold_in(key_of[15], 71), 0)
    time_step = draw_time_step(jax.random.fold_in(key_of[15], 71), 0)
    damping = draw_damping(jax.random.fold_in(key_of[15], 71), 0)
    input_map = normal_values(key_of[3], (2, 2, G, STATE, GROUP), (2 * GROUP) ** -0.5, 1.0, ((2, 4),))
    readout = normal_values(key_of[4], (2, 2, G, GROUP, STATE), (2 * STATE) ** -0.5, 0.5, ((2, 4),), jnp.float32)
    skip_gain = normal_values(key_of[5], (DS,), 1.0, 4.0, ((0, 4),), jnp.float32)
    out_gain = jnp.clip(1.0 + 0.18 * jax.random.normal(key_of[6], (DS,), jnp.float32), 0.1, 1.9)
    out_weight = normal_values(key_of[7], (DS, D), DS ** -0.5, 0.1875)
    residual = normal_values(key_of[8], (TOKEN_POSITIONS, D), 1.0, 6.0, ((0, 32),))
    channel_gain = jnp.clip(1.0 + 0.18 * jax.random.normal(key_of[9], (D,), jnp.float32), 0.1, 1.9)
    value_weight = normal_values(key_of[10], (D, FF), D ** -0.5, 0.125, ((0, 8), (1, 4)))
    gate_weight = normal_values(key_of[11], (D, FF), D ** -0.5, 0.125, ((0, 8), (1, 4)))
    value_taps = normal_values(key_of[12], (3, FF), 0.577, 3.0, ((1, 4),), jnp.float32)
    gate_taps = normal_values(key_of[13], (3, FF), 0.577, 3.0, ((1, 4),), jnp.float32)
    down_weight = normal_values(key_of[14], (FF, D), FF ** -0.5, 0.078125, ((0, 4), (1, 8)))
    return dict(mixer_input=mixer_input, time_step=time_step, damping=damping, input_map=input_map, readout=readout, skip_gain=skip_gain, out_gain=out_gain, out_weight=out_weight, residual=residual, channel_gain=channel_gain, value_weight=value_weight, gate_weight=gate_weight, value_taps=value_taps, gate_taps=gate_taps, down_weight=down_weight)


norm_eps = 1e-06
highest = lax.Precision.HIGHEST

def combine(earlier, latter):
    prod_real = latter[0] * earlier[0] - latter[1] * earlier[1]
    prod_imag = latter[0] * earlier[1] + latter[1] * earlier[0]
    sum_real = latter[0] * earlier[2] - latter[1] * earlier[3] + latter[2]
    sum_imag = latter[0] * earlier[3] + latter[1] * earlier[2] + latter[3]
    return (prod_real, prod_imag, sum_real, sum_imag)

def group_mixer(operands):
    group_input, step_pair, damp_pair, in_maps, out_maps = operands
    states = in_maps.shape[2]
    frequency = math.pi * jnp.arange(states, dtype=jnp.float32)
    result = jnp.zeros(group_input.shape, jnp.float32)
    for direction in range(2):
        step_size = step_pair[direction]
        rotation = step_size * frequency
        magnitude = jnp.exp(-0.5 * step_size - damp_pair[direction])[:, None]
        decay_real = magnitude * jnp.cos(rotation)[None, :]
        decay_imag = magnitude * jnp.sin(rotation)[None, :]
        in_scale = jnp.sqrt(-jnp.expm1(-step_size))
        drive_real = jnp.dot(group_input, in_maps[direction, 0].T, preferred_element_type=jnp.float32) * in_scale
        drive_imag = jnp.dot(group_input, in_maps[direction, 1].T, preferred_element_type=jnp.float32) * in_scale
        scanned = lax.associative_scan(combine, (decay_real, decay_imag, drive_real, drive_imag), reverse=direction == 1, axis=0)
        result = result + jnp.dot(scanned[2], out_maps[direction, 0].T, precision=highest)
        result = result - jnp.dot(scanned[3], out_maps[direction, 1].T, precision=highest)
    return result

def shifted_sum(values, tap_rows):
    widened = jnp.pad(values.astype(jnp.float32), ((1, 1), (0, 0)))
    return tap_rows[0] * widened[:-2] + tap_rows[1] * widened[1:-1] + tap_rows[2] * widened[2:]

def reference(mixer_input, time_step, damping, input_map, readout, skip_gain, out_gain, out_weight, residual, channel_gain, value_weight, gate_weight, value_taps, gate_taps, down_weight):
    tokens, channels = mixer_input.shape
    group_count = time_step.shape[1]
    group_width = channels // group_count
    grouped = jnp.transpose(mixer_input.reshape(tokens, group_count, group_width), (1, 0, 2))
    per_group = lax.map(group_mixer, (grouped, time_step.T, jnp.transpose(damping, (2, 0, 1)), jnp.moveaxis(input_map, 2, 0), jnp.moveaxis(readout, 2, 0)))
    mixed_y = jnp.transpose(per_group, (1, 0, 2)).reshape(tokens, channels) + skip_gain[None, :] * mixer_input.astype(jnp.float32)
    inverse = lax.rsqrt(lax.optimization_barrier(jnp.mean(mixed_y * mixed_y, axis=1, keepdims=True)) + norm_eps)
    normed_mix = (mixed_y * inverse * out_gain[None, :]).astype(jnp.bfloat16)
    mixed_rows = jnp.dot(normed_mix, out_weight, preferred_element_type=jnp.float32)
    hidden_state = (residual.astype(jnp.float32) + mixed_rows).astype(jnp.bfloat16)
    state_wide = hidden_state.astype(jnp.float32)
    scale_rows = lax.rsqrt(lax.optimization_barrier(jnp.mean(state_wide * state_wide, axis=1, keepdims=True)) + norm_eps)
    normed = (state_wide * scale_rows * channel_gain[None, :]).astype(jnp.bfloat16)
    value_up = jnp.dot(normed, value_weight, preferred_element_type=jnp.float32).astype(jnp.bfloat16)
    gate_up = jnp.dot(normed, gate_weight, preferred_element_type=jnp.float32).astype(jnp.bfloat16)
    value_conv = shifted_sum(value_up, value_taps)
    gate_conv = shifted_sum(gate_up, gate_taps)
    hidden = (value_conv * jax.nn.silu(gate_conv)).astype(jnp.bfloat16)
    block_width = FF // N_TP
    summed = jnp.zeros((tokens, out_weight.shape[1]), jnp.float32)
    for part_index in range(N_TP):
        first_col = part_index * block_width
        partial_value = jnp.dot(hidden[:, first_col:first_col + block_width], down_weight[first_col:first_col + block_width], preferred_element_type=jnp.float32)
        rounded = lax.optimization_barrier(partial_value.astype(jnp.bfloat16))
        summed = summed + rounded.astype(jnp.float32)
    return (state_wide + summed).astype(jnp.bfloat16)
```

```python
import math

import jax
import jax.numpy as jnp
from jax import lax
from jax.experimental import pallas as pl
from jax.experimental.pallas import tpu as pltpu
from jax.sharding import PartitionSpec as P

norm_eps = 1e-06
highest = lax.Precision.HIGHEST
f32 = jnp.float32
bf16 = jnp.bfloat16


def split2(a):
    top = a.astype(bf16)
    return top, (a - top.astype(f32)).astype(bf16)


def dot3(a, b):
    a0, a1 = split2(a)
    b0, b1 = split2(b)
    total = jnp.dot(a0, b0, preferred_element_type=f32)
    total += jnp.dot(a0, b1, preferred_element_type=f32)
    return total + jnp.dot(a1, b0, preferred_element_type=f32)


def cos_sin(coarse, fine, count):
    first = coarse * count
    first = first - jnp.floor(first + 0.5)
    turn = first + fine * count
    half = jnp.floor(2.0 * turn + 0.5)
    angle = (2.0 * math.pi) * (turn - 0.5 * half)
    odd = half - 2.0 * jnp.floor(0.5 * half)
    sign = 1.0 - 2.0 * odd
    z = angle * angle
    sine = jnp.full_like(z, -1.0 / 39916800.0)
    for c in (1.0 / 362880.0, -1.0 / 5040.0, 1.0 / 120.0, -1.0 / 6.0, 1.0):
        sine = sine * z + c
    cosine = jnp.full_like(z, 1.0 / 479001600.0)
    for c in (-1.0 / 3628800.0, 1.0 / 40320.0, -1.0 / 720.0, 1.0 / 24.0, -0.5, 1.0):
        cosine = cosine * z + c
    return cosine * sign, sine * (angle * sign)


def iota(shape, dim):
    return lax.broadcasted_iota(jnp.int32, shape, dim)


def turns_of(states, rows, backward):
    when = iota((states, rows), 1)
    when = rows - 1 - when if backward else when
    return (iota((states, rows), 0) * when).astype(f32)


def local_kernel(scal, xt, damp, in_map, readout, yt, ends, rows_a):
    groups, rows = damp.shape[1], damp.shape[2]
    states, chans = in_map.shape[3], in_map.shape[4]
    part, quarter = states // 2, 2 * groups
    lane = iota((part, ends.shape[1]), 1)
    row_id, col_id = iota((rows, rows), 0), iota((rows, rows), 1)
    kept = (row_id <= col_id, row_id >= col_id)
    for k in range(2):
        rows_a[k] = jnp.dot(damp[k], kept[k].astype(f32), precision=highest)
    counts = [turns_of(states, rows, k == 1) for k in range(2)]

    def group(g, held):
        at = pl.ds(pl.multiple_of(g * chans, chans), chans)
        x = xt[at, :]
        total = jnp.zeros((chans, rows), f32)
        for k in range(2):
            cosine, sine = cos_sin(scal[0, k, g], scal[1, k, g], counts[k])
            scale = scal[2, k, g]
            drive_r = jnp.dot(in_map[k, 0, g], x, preferred_element_type=f32) * scale
            drive_i = jnp.dot(in_map[k, 1, g], x, preferred_element_type=f32) * scale
            turned = jnp.concatenate(
                (cosine * drive_r + sine * drive_i, cosine * drive_i - sine * drive_r), axis=0
            )
            across = jnp.broadcast_to(rows_a[k, pl.ds(g, 1), :], (rows, rows))
            decay = jnp.exp(jnp.where(kept[k], across.T - across, -1e30))
            z = dot3(turned, decay)
            z_r, z_i = z[:states], z[states:]
            s_r = cosine * z_r - sine * z_i
            s_i = cosine * z_i + sine * z_r
            total += dot3(readout[k, 0, g], s_r) - dot3(readout[k, 1, g], s_i)
            last = 0 if k else rows - 1
            for p, s in enumerate((s_r, s_i)):
                col = s[:, last : last + 1]
                for half in range(2):
                    spot = (half * 2 + p) * quarter + k * groups + g
                    held = jnp.where(lane == spot, col[half * part : (half + 1) * part], held)
        yt[at, :] = total
        return held

    held = lax.fori_loop(0, groups, group, jnp.zeros((part, ends.shape[1]), f32))
    ends[...] = held


def carry_kernel(scal, place, xt, rows_a, lanes, every, readout, yt, skip, gain, out):
    groups, rows = rows_a.shape[1], rows_a.shape[2]
    chans, states = readout.shape[3], readout.shape[4]
    blocks = every.shape[0]
    part, quarter = states // 2, 2 * groups
    mine = place[0]
    number = iota((states, quarter), 0).astype(f32)
    backward = iota((states, quarter), 1) >= groups
    coarse, fine = lanes[0:1, :], lanes[1:2, :]
    far_r, far_i = cos_sin(coarse, fine, number * rows)
    near_r, near_i = cos_sin(coarse, fine, number)
    def piece(b, p):
        ref = every.at[b]
        return jnp.concatenate(
            [ref[:part, (h * 2 + p) * quarter : (h * 2 + p + 1) * quarter] for h in range(2)], axis=0
        )

    c_r = jnp.zeros((states, quarter), f32)
    c_i = jnp.zeros((states, quarter), f32)
    for b in range(blocks - 1):
        other = blocks - 1 - b
        e_r = jnp.where(backward, piece(other, 0), piece(b, 0))
        e_i = jnp.where(backward, piece(other, 1), piece(b, 1))
        span = jnp.where(
            backward[:1], every[other, part : part + 1, :quarter], every[b, part : part + 1, :quarter]
        )
        fade = jnp.exp(-span)
        n_r = fade * (far_r * c_r - far_i * c_i) + e_r
        n_i = fade * (far_r * c_i + far_i * c_r) + e_i
        place_in = jnp.where(backward, blocks - 1 - mine, mine)
        c_r = jnp.where(b < place_in, n_r, c_r)
        c_i = jnp.where(b < place_in, n_i, c_i)
    w_r = near_r * c_r - near_i * c_i
    w_i = near_r * c_i + near_i * c_r
    counts = [turns_of(states, rows, k == 1) for k in range(2)]
    squares = jnp.zeros((8, rows), f32)
    for g in range(groups):
        at = pl.ds(g * chans, chans)
        total = yt[at, :] + skip[at, :] * xt[at, :].astype(f32)
        for k in range(2):
            cosine, sine = cos_sin(scal[0, k, g], scal[1, k, g], counts[k])
            l = k * groups + g
            a, b = w_r[:, l : l + 1], w_i[:, l : l + 1]
            fade = jnp.exp(-rows_a[k, g : g + 1, :])
            s_r = (cosine * a - sine * b) * fade
            s_i = (cosine * b + sine * a) * fade
            total += dot3(readout[k, 0, g], s_r) - dot3(readout[k, 1, g], s_i)
        for r in range(0, chans, 8):
            squares += total[r : r + 8] * total[r : r + 8]
        out[at, :] = (total * gain[at, :]).astype(bf16)
    square = jnp.sum(squares, axis=0, keepdims=True)
    top = square.astype(bf16)
    rest = square - top.astype(f32)
    mid = rest.astype(bf16)
    low = (rest - mid.astype(f32)).astype(bf16)
    extra = out.shape[0] - groups * chans
    which = iota((extra, rows), 0)
    tail = jnp.where(which == 0, top.astype(f32), jnp.where(which == 1, mid.astype(f32), low.astype(f32)))
    tail = jnp.where(which < 3, tail, 0.0)
    out[pl.ds(groups * chans, extra), :] = tail.astype(bf16)


square_rows = 16


def vmem(count):
    return [pl.BlockSpec(memory_space=pltpu.VMEM)] * count


def mixer_local(mixer_input, time_step, damping, input_map, readout):
    rows, width = mixer_input.shape
    groups = time_step.shape[1]
    states = input_map.shape[3]
    half_step = 0.5 * time_step
    coarse = jnp.floor(half_step * 2048.0) / 2048.0
    scal = jnp.stack((coarse, half_step - coarse, jnp.sqrt(-jnp.expm1(-time_step))))
    damp = jnp.swapaxes(damping, 1, 2) + half_step[:, :, None]
    xt = mixer_input.T
    lanes = 8 * groups
    smem = pl.BlockSpec(memory_space=pltpu.SMEM)
    yt, ends, rows_a = pl.pallas_call(
        local_kernel,
        out_shape=(
            jax.ShapeDtypeStruct((width, rows), f32),
            jax.ShapeDtypeStruct((states // 2, lanes), f32),
            jax.ShapeDtypeStruct(damp.shape, f32),
        ),
        in_specs=[smem] + vmem(4),
        out_specs=tuple(vmem(3)),
        name="mixer_local",
    )(scal, xt, damp, input_map, readout)
    span = jnp.sum(damp, axis=2).reshape(1, -1)
    extra = jnp.zeros((8, lanes), f32).at[:1, : span.shape[1]].set(span)
    return scal, xt, yt, rows_a, jnp.concatenate((ends, extra), axis=0)


def mixer_carried(scal, xt, yt, rows_a, every, readout, skip_gain, out_gain):
    width, rows = xt.shape
    smem = pl.BlockSpec(memory_space=pltpu.SMEM)
    place = lax.axis_index("sp").reshape(1)
    lanes = scal[:2].reshape(2, -1)
    return pl.pallas_call(
        carry_kernel,
        out_shape=jax.ShapeDtypeStruct((width + square_rows, rows), bf16),
        in_specs=[smem, smem] + vmem(8),
        out_specs=pl.BlockSpec(memory_space=pltpu.VMEM),
        name="mixer_carried",
    )(scal, place, xt, rows_a, lanes, every, readout, yt, skip_gain[:, None], out_gain[:, None])


def with_halo(cells, axis):
    count = lax.axis_size(axis)
    return jnp.concatenate(
        [
            lax.ppermute(cells[-1:], axis, [(i, i + 1) for i in range(count - 1)]),
            cells,
            lax.ppermute(cells[:1], axis, [(i + 1, i) for i in range(count - 1)]),
        ],
        axis=0,
    )


def body(
    mixer_input,
    time_step,
    damping,
    input_map,
    readout,
    skip_gain,
    out_gain,
    out_weight,
    residual,
    channel_gain,
    value_weight,
    gate_weight,
    value_taps,
    gate_taps,
    down_weight,
):
    tp_count, sp_count = lax.axis_size("tp"), lax.axis_size("sp")
    tok_rows, local_width = mixer_input.shape
    residual_rows = lax.all_gather(residual, "tp", axis=0, tiled=True)
    scal, xt, yt, rows_a, ends = mixer_local(mixer_input, time_step, damping, input_map, readout)
    every = lax.all_to_all(
        jnp.broadcast_to(ends[None], (sp_count,) + ends.shape), "sp", 0, 0, tiled=True
    )
    mixed = mixer_carried(scal, xt, yt, rows_a, every, readout, skip_gain, out_gain)
    mixed = lax.all_gather(mixed, "tp", axis=0)
    squares = jnp.sum(mixed[:, local_width:].astype(f32), axis=(0, 1))
    inverse = lax.rsqrt(squares / (local_width * tp_count) + norm_eps)
    channels = mixed[:, :local_width].reshape(local_width * tp_count, tok_rows)
    mixed_rows = (
        lax.dot_general(channels, out_weight, (((0,), (0,)), ((), ())), preferred_element_type=f32)
        * inverse[:, None]
    )
    hidden_state = (residual_rows.astype(f32) + mixed_rows).astype(bf16)
    state_wide = hidden_state.astype(f32)
    scale_rows = lax.rsqrt(jnp.mean(state_wide * state_wide, axis=1, keepdims=True) + norm_eps)
    block_rows = (state_wide * scale_rows * channel_gain[None, :]).astype(bf16)
    hidden_width = value_weight.shape[1]
    value_up = jnp.dot(
        block_rows,
        lax.all_gather(value_weight, "sp", axis=0, tiled=True),
        preferred_element_type=f32,
    )
    gate_up = jnp.dot(
        block_rows,
        lax.all_gather(gate_weight, "sp", axis=0, tiled=True),
        preferred_element_type=f32,
    )
    both_up = jnp.concatenate((value_up.astype(bf16), gate_up.astype(bf16)), axis=1)
    padded = with_halo(both_up, "sp")
    taps = jnp.concatenate((value_taps, gate_taps), axis=1)
    convolved = (
        taps[0] * padded[:-2].astype(f32)
        + taps[1] * padded[1:-1].astype(f32)
        + taps[2] * padded[2:].astype(f32)
    )
    hidden = (convolved[:, :hidden_width] * jax.nn.silu(convolved[:, hidden_width:])).astype(bf16)
    down_full = lax.all_gather(down_weight, "sp", axis=1, tiled=True)
    partial = jnp.dot(hidden, down_full, preferred_element_type=f32).astype(bf16)
    pieces = lax.all_to_all(
        partial.reshape(tp_count, tok_rows // tp_count, -1), "tp", 0, 0, tiled=True
    )
    mine = lax.axis_index("tp") * (tok_rows // tp_count)
    own = lax.dynamic_slice_in_dim(state_wide, mine, tok_rows // tp_count, axis=0)
    return (own + jnp.sum(pieces.astype(f32), axis=0)).astype(bf16)


def solution(mesh):
    in_specs = (
        P("sp", "tp"),
        P(None, "tp"),
        P(None, "sp", "tp"),
        P(None, None, "tp", None, None),
        P(None, None, "tp", None, None),
        P("tp"),
        P("tp"),
        P(),
        P(("sp", "tp"), None),
        P(),
        P("sp", "tp"),
        P("sp", "tp"),
        P(None, "tp"),
        P(None, "tp"),
        P("tp", "sp"),
    )
    out_specs = P(("sp", "tp"), None)
    return jax.shard_map(body, mesh=mesh, in_specs=in_specs, out_specs=out_specs, check_vma=False)
```

```python
import math

import jax
import jax.numpy as jnp
from jax import lax
from jax.experimental import pallas as pl
from jax.experimental.pallas import tpu as pltpu
from jax.sharding import PartitionSpec as P

norm_eps = 1e-06
highest = lax.Precision.HIGHEST
f32 = jnp.float32
bf16 = jnp.bfloat16


def split2(a):
    top = a.astype(bf16)
    return top, (a - top.astype(f32)).astype(bf16)


def dot3(a, b):
    a0, a1 = split2(a)
    b0, b1 = split2(b)
    total = jnp.dot(a0, b0, preferred_element_type=f32)
    total += jnp.dot(a0, b1, preferred_element_type=f32)
    return total + jnp.dot(a1, b0, preferred_element_type=f32)


def cos_sin(coarse, fine, count):
    first = coarse * count
    first = first - jnp.floor(first + 0.5)
    turn = first + fine * count
    half = jnp.floor(2.0 * turn + 0.5)
    angle = (2.0 * math.pi) * (turn - 0.5 * half)
    odd = half - 2.0 * jnp.floor(0.5 * half)
    sign = 1.0 - 2.0 * odd
    z = angle * angle
    sine = jnp.full_like(z, -1.0 / 39916800.0)
    for c in (1.0 / 362880.0, -1.0 / 5040.0, 1.0 / 120.0, -1.0 / 6.0, 1.0):
        sine = sine * z + c
    cosine = jnp.full_like(z, 1.0 / 479001600.0)
    for c in (-1.0 / 3628800.0, 1.0 / 40320.0, -1.0 / 720.0, 1.0 / 24.0, -0.5, 1.0):
        cosine = cosine * z + c
    return cosine * sign, sine * (angle * sign)


def iota(shape, dim):
    return lax.broadcasted_iota(jnp.int32, shape, dim)


def turns_of(states, rows, backward):
    when = iota((states, rows), 1)
    when = rows - 1 - when if backward else when
    return (iota((states, rows), 0) * when).astype(f32)


def local_kernel(scal, xt, damp, in_map, readout, yt, ends, rows_a):
    groups, rows = damp.shape[1], damp.shape[2]
    states, chans = in_map.shape[3], in_map.shape[4]
    part, quarter = states // 2, 2 * groups
    lane = iota((part, ends.shape[1]), 1)
    row_id, col_id = iota((rows, rows), 0), iota((rows, rows), 1)
    kept = (row_id <= col_id, row_id >= col_id)
    for k in range(2):
        rows_a[k] = jnp.dot(damp[k], kept[k].astype(f32), precision=highest)
    counts = [turns_of(states, rows, k == 1) for k in range(2)]

    def group(g, held):
        at = pl.ds(pl.multiple_of(g * chans, chans), chans)
        x = xt[at, :]
        total = jnp.zeros((chans, rows), f32)
        for k in range(2):
            cosine, sine = cos_sin(scal[0, k, g], scal[1, k, g], counts[k])
            scale = scal[2, k, g]
            drive_r = jnp.dot(in_map[k, 0, g], x, preferred_element_type=f32) * scale
            drive_i = jnp.dot(in_map[k, 1, g], x, preferred_element_type=f32) * scale
            turned = jnp.concatenate(
                (cosine * drive_r + sine * drive_i, cosine * drive_i - sine * drive_r), axis=0
            )
            across = jnp.broadcast_to(rows_a[k, pl.ds(g, 1), :], (rows, rows))
            decay = jnp.exp(jnp.where(kept[k], across.T - across, -1e30))
            z = dot3(turned, decay)
            z_r, z_i = z[:states], z[states:]
            s_r = cosine * z_r - sine * z_i
            s_i = cosine * z_i + sine * z_r
            total += dot3(readout[k, 0, g], s_r) - dot3(readout[k, 1, g], s_i)
            last = 0 if k else rows - 1
            for p, s in enumerate((s_r, s_i)):
                col = s[:, last : last + 1]
                for half in range(2):
                    spot = (half * 2 + p) * quarter + k * groups + g
                    held = jnp.where(lane == spot, col[half * part : (half + 1) * part], held)
        yt[at, :] = total
        return held

    held = lax.fori_loop(0, groups, group, jnp.zeros((part, ends.shape[1]), f32))
    ends[...] = held


def carry_kernel(scal, place, xt, rows_a, lanes, every, readout, yt, skip, gain, out):
    groups, rows = rows_a.shape[1], rows_a.shape[2]
    chans, states = readout.shape[3], readout.shape[4]
    blocks = every.shape[0]
    part, quarter = states // 2, 2 * groups
    mine = place[0]
    number = iota((states, quarter), 0).astype(f32)
    backward = iota((states, quarter), 1) >= groups
    coarse, fine = lanes[0:1, :], lanes[1:2, :]
    far_r, far_i = cos_sin(coarse, fine, number * rows)
    near_r, near_i = cos_sin(coarse, fine, number)
    def piece(b, p):
        ref = every.at[b]
        return jnp.concatenate(
            [ref[:part, (h * 2 + p) * quarter : (h * 2 + p + 1) * quarter] for h in range(2)], axis=0
        )

    c_r = jnp.zeros((states, quarter), f32)
    c_i = jnp.zeros((states, quarter), f32)
    for b in range(blocks - 1):
        other = blocks - 1 - b
        e_r = jnp.where(backward, piece(other, 0), piece(b, 0))
        e_i = jnp.where(backward, piece(other, 1), piece(b, 1))
        span = jnp.where(
            backward[:1], every[other, part : part + 1, :quarter], every[b, part : part + 1, :quarter]
        )
        fade = jnp.exp(-span)
        n_r = fade * (far_r * c_r - far_i * c_i) + e_r
        n_i = fade * (far_r * c_i + far_i * c_r) + e_i
        place_in = jnp.where(backward, blocks - 1 - mine, mine)
        c_r = jnp.where(b < place_in, n_r, c_r)
        c_i = jnp.where(b < place_in, n_i, c_i)
    w_r = near_r * c_r - near_i * c_i
    w_i = near_r * c_i + near_i * c_r
    counts = [turns_of(states, rows, k == 1) for k in range(2)]
    squares = jnp.zeros((8, rows), f32)
    for g in range(groups):
        at = pl.ds(g * chans, chans)
        total = yt[at, :] + skip[at, :] * xt[at, :].astype(f32)
        for k in range(2):
            cosine, sine = cos_sin(scal[0, k, g], scal[1, k, g], counts[k])
            l = k * groups + g
            a, b = w_r[:, l : l + 1], w_i[:, l : l + 1]
            fade = jnp.exp(-rows_a[k, g : g + 1, :])
            s_r = (cosine * a - sine * b) * fade
            s_i = (cosine * b + sine * a) * fade
            total += dot3(readout[k, 0, g], s_r) - dot3(readout[k, 1, g], s_i)
        for r in range(0, chans, 8):
            squares += total[r : r + 8] * total[r : r + 8]
        out[at, :] = (total * gain[at, :]).astype(bf16)
    square = jnp.sum(squares, axis=0, keepdims=True)
    top = square.astype(bf16)
    rest = square - top.astype(f32)
    mid = rest.astype(bf16)
    low = (rest - mid.astype(f32)).astype(bf16)
    extra = out.shape[0] - groups * chans
    which = iota((extra, rows), 0)
    tail = jnp.where(which == 0, top.astype(f32), jnp.where(which == 1, mid.astype(f32), low.astype(f32)))
    tail = jnp.where(which < 3, tail, 0.0)
    out[pl.ds(groups * chans, extra), :] = tail.astype(bf16)


square_rows = 16


def vmem(count):
    return [pl.BlockSpec(memory_space=pltpu.VMEM)] * count


def mixer_local(mixer_input, time_step, damping, input_map, readout):
    rows, width = mixer_input.shape
    groups = time_step.shape[1]
    states = input_map.shape[3]
    half_step = 0.5 * time_step
    coarse = jnp.floor(half_step * 2048.0) / 2048.0
    scal = jnp.stack((coarse, half_step - coarse, jnp.sqrt(-jnp.expm1(-time_step))))
    damp = jnp.swapaxes(damping, 1, 2) + half_step[:, :, None]
    xt = mixer_input.T
    lanes = 8 * groups
    smem = pl.BlockSpec(memory_space=pltpu.SMEM)
    yt, ends, rows_a = pl.pallas_call(
        local_kernel,
        out_shape=(
            jax.ShapeDtypeStruct((width, rows), f32),
            jax.ShapeDtypeStruct((states // 2, lanes), f32),
            jax.ShapeDtypeStruct(damp.shape, f32),
        ),
        in_specs=[smem] + vmem(4),
        out_specs=tuple(vmem(3)),
        name="mixer_local",
    )(scal, xt, damp, input_map, readout)
    span = jnp.sum(damp, axis=2).reshape(1, -1)
    extra = jnp.zeros((8, lanes), f32).at[:1, : span.shape[1]].set(span)
    return scal, xt, yt, rows_a, jnp.concatenate((ends, extra), axis=0)


def mixer_carried(scal, xt, yt, rows_a, every, readout, skip_gain, out_gain):
    width, rows = xt.shape
    smem = pl.BlockSpec(memory_space=pltpu.SMEM)
    place = lax.axis_index("sp").reshape(1)
    lanes = scal[:2].reshape(2, -1)
    return pl.pallas_call(
        carry_kernel,
        out_shape=jax.ShapeDtypeStruct((width + square_rows, rows), bf16),
        in_specs=[smem, smem] + vmem(8),
        out_specs=pl.BlockSpec(memory_space=pltpu.VMEM),
        name="mixer_carried",
    )(scal, place, xt, rows_a, lanes, every, readout, yt, skip_gain[:, None], out_gain[:, None])


def with_halo(cells, axis):
    count = lax.axis_size(axis)
    return jnp.concatenate(
        [
            lax.ppermute(cells[-1:], axis, [(i, i + 1) for i in range(count - 1)]),
            cells,
            lax.ppermute(cells[:1], axis, [(i + 1, i) for i in range(count - 1)]),
        ],
        axis=0,
    )


def gathered_body(
    mixer_input,
    time_step,
    damping,
    input_map,
    readout,
    skip_gain,
    out_gain,
    out_weight,
    residual,
    channel_gain,
    value_weight,
    gate_weight,
    value_taps,
    gate_taps,
    down_weight,
):
    tp_count, sp_count = lax.axis_size("tp"), lax.axis_size("sp")
    tok_rows, local_width = mixer_input.shape
    residual_rows = lax.all_gather(residual, "tp", axis=0, tiled=True)
    scal, xt, yt, rows_a, ends = mixer_local(mixer_input, time_step, damping, input_map, readout)
    every = lax.all_to_all(
        jnp.broadcast_to(ends[None], (sp_count,) + ends.shape), "sp", 0, 0, tiled=True
    )
    mixed = mixer_carried(scal, xt, yt, rows_a, every, readout, skip_gain, out_gain)
    mixed = lax.all_gather(mixed, "tp", axis=0)
    squares = jnp.sum(mixed[:, local_width:].astype(f32), axis=(0, 1))
    inverse = lax.rsqrt(squares / (local_width * tp_count) + norm_eps)
    channels = mixed[:, :local_width].reshape(local_width * tp_count, tok_rows)
    mixed_rows = (
        lax.dot_general(channels, out_weight, (((0,), (0,)), ((), ())), preferred_element_type=f32)
        * inverse[:, None]
    )
    hidden_state = (residual_rows.astype(f32) + mixed_rows).astype(bf16)
    state_wide = hidden_state.astype(f32)
    scale_rows = lax.rsqrt(jnp.mean(state_wide * state_wide, axis=1, keepdims=True) + norm_eps)
    block_rows = (state_wide * scale_rows * channel_gain[None, :]).astype(bf16)
    hidden_width = value_weight.shape[1]
    value_up = jnp.dot(
        block_rows,
        lax.all_gather(value_weight, "sp", axis=0, tiled=True),
        preferred_element_type=f32,
    )
    gate_up = jnp.dot(
        block_rows,
        lax.all_gather(gate_weight, "sp", axis=0, tiled=True),
        preferred_element_type=f32,
    )
    both_up = jnp.concatenate((value_up.astype(bf16), gate_up.astype(bf16)), axis=1)
    padded = with_halo(both_up, "sp")
    taps = jnp.concatenate((value_taps, gate_taps), axis=1)
    convolved = (
        taps[0] * padded[:-2].astype(f32)
        + taps[1] * padded[1:-1].astype(f32)
        + taps[2] * padded[2:].astype(f32)
    )
    hidden = (convolved[:, :hidden_width] * jax.nn.silu(convolved[:, hidden_width:])).astype(bf16)
    down_full = lax.all_gather(down_weight, "sp", axis=1, tiled=True)
    partial = jnp.dot(hidden, down_full, preferred_element_type=f32).astype(bf16)
    pieces = lax.all_to_all(
        partial.reshape(tp_count, tok_rows // tp_count, -1), "tp", 0, 0, tiled=True
    )
    mine = lax.axis_index("tp") * (tok_rows // tp_count)
    own = lax.dynamic_slice_in_dim(state_wide, mine, tok_rows // tp_count, axis=0)
    return (own + jnp.sum(pieces.astype(f32), axis=0)).astype(bf16)


def ring(axis, inner, step, low=0):
    size = lax.axis_size(axis)
    outer = size // inner
    return [
        (i, ((i // inner + step) % outer) * inner + (i + low) % inner) for i in range(size)
    ]


def outer_send(pick, axis, inner):
    outer = lax.axis_size(axis) // inner
    return [lax.ppermute(pick(s), axis, ring(axis, inner, s)) for s in range(1, outer)]


def spread(slices):
    outer = slices.shape[0]
    mine = lax.axis_index("sp") // pair

    def pick(step):
        return lax.dynamic_index_in_dim(slices, lax.rem(mine + step, outer), 0, False)

    own = jnp.stack([pick(0)] + outer_send(pick, "sp", pair))
    beside = lax.ppermute(own, "sp", ring("sp", pair, 0, 1))
    over = ring("tp", pair, 0, 1)
    return own, beside, lax.ppermute(own, "tp", over), lax.ppermute(beside, "tp", over)


pair = 2


def row_block(outer, which, step):
    sp = lax.axis_index("sp")
    far = lax.rem(sp // pair + outer - step, outer)
    return far * pair + lax.rem(sp + which, pair)


def up_kernel(x, *refs):
    stacks, (out, full, sems) = refs[:8], refs[8:]
    outer, rows, cols = stacks[0].shape
    groups = []
    for kind in range(2):
        for core in range(2):
            copies = []
            for which in range(2):
                ref = stacks[kind * 4 + core * 2 + which]
                for s in range(outer):
                    first = pl.multiple_of(row_block(outer, which, s) * rows, rows)
                    slot = kind * 2 + core
                    copy = pltpu.make_async_copy(
                        ref.at[s],
                        full.at[slot, pl.ds(first, rows), :],
                        sems.at[slot, which * outer + s],
                    )
                    copy.start()
                    copies.append(copy)
            groups.append(copies)
    for slot, copies in enumerate(groups):
        for copy in copies:
            copy.wait()
        out[:, slot * cols : (slot + 1) * cols] = jnp.dot(
            x[...], full[slot], preferred_element_type=f32
        ).astype(bf16)


def down_kernel(up, before, after, taps, *refs):
    stacks, (out, full, sems) = refs[:4], refs[4:]
    outer, rows, cols = stacks[0].shape
    copies = []
    for core in range(2):
        for which in range(2):
            ref = stacks[core * 2 + which]
            for s in range(outer):
                first = pl.multiple_of(row_block(outer, which, s) * cols, cols)
                copy = pltpu.make_async_copy(
                    ref.at[s],
                    full.at[pl.ds(core * rows, rows), pl.ds(first, cols)],
                    sems.at[core * 2 + which, s],
                )
                copy.start()
                copies.append(copy)
    width = 2 * rows
    count, pieces = up.shape[0], before.shape[0]
    length = count // pieces

    def convolved(start):
        at = slice(start, start + width)
        rows_id = iota((length, width), 0)
        done = []
        for p in range(pieces):
            cells = up[p * length : (p + 1) * length, at].astype(f32)
            left = pltpu.roll(cells, 1, 0)
            left = jnp.where(rows_id == 0, before[p : p + 1, at].astype(f32), left)
            right = pltpu.roll(cells, length - 1, 0)
            right = jnp.where(rows_id == length - 1, after[p : p + 1, at].astype(f32), right)
            done.append(taps[0:1, at] * left + taps[1:2, at] * cells + taps[2:3, at] * right)
        return jnp.concatenate(done, axis=0)

    gate = convolved(width)
    hidden = (convolved(0) * (gate / (1.0 + jnp.exp(-gate)))).astype(bf16)
    for copy in copies:
        copy.wait()
    out[...] = jnp.dot(hidden, full[...], preferred_element_type=f32).astype(bf16)


def up_projection(x, stacks):
    outer, rows, cols = stacks[0].shape
    return pl.pallas_call(
        up_kernel,
        out_shape=jax.ShapeDtypeStruct((x.shape[0], 4 * cols), bf16),
        in_specs=vmem(1) + [pl.BlockSpec(memory_space=pltpu.HBM)] * 8,
        out_specs=pl.BlockSpec(memory_space=pltpu.VMEM),
        scratch_shapes=[
            pltpu.VMEM((4, 2 * outer * rows, cols), bf16),
            pltpu.SemaphoreType.DMA((4, 2 * outer)),
        ],
        name="up_projection",
    )(x, *stacks)


def down_projection(up, before, after, taps, stacks):
    outer, rows, cols = stacks[0].shape
    return pl.pallas_call(
        down_kernel,
        out_shape=jax.ShapeDtypeStruct((up.shape[0], 2 * outer * cols), bf16),
        in_specs=vmem(4) + [pl.BlockSpec(memory_space=pltpu.HBM)] * 4,
        out_specs=pl.BlockSpec(memory_space=pltpu.VMEM),
        scratch_shapes=[
            pltpu.VMEM((2 * rows, 2 * outer * cols), bf16),
            pltpu.SemaphoreType.DMA((4, outer)),
        ],
        name="down_projection",
    )(up, before, after, taps, *stacks)


def edges_of(up, outer, inner):
    sp, tp = lax.axis_index("sp"), lax.axis_index("tp")
    z, y, x, c = sp // pair, lax.rem(sp, pair), tp // pair, lax.rem(tp, pair)
    cells = up.reshape(outer, inner, -1, 2, 2, up.shape[1] // 4)[:, :, :, :, ::-1]
    cells = cells.reshape(outer, inner, -1, up.shape[1])
    ends = jnp.stack((cells[:, :, 0], cells[:, :, -1]))
    across = lax.ppermute(ends, "tp", ring("tp", pair, 0, 1))
    rim = jnp.where(c == 0, lax.rem(inner - x, inner), inner - 1 - x)
    out_edge = lax.dynamic_index_in_dim(
        lax.dynamic_index_in_dim(ends, c, 0, False), rim, 1, False
    )
    sizes = (lax.axis_size("sp"), lax.axis_size("tp"))
    hops = [
        (i * sizes[1] + j, (i ^ 1) * sizes[1] + (j ^ 1))
        for i in range(sizes[0])
        for j in range(sizes[1])
    ]
    rim_rows = lax.ppermute(out_edge, ("sp", "tp"), hops)
    block = lax.rem(z + outer - jnp.arange(outer), outer)
    before_rim = jnp.where(y == 0, jnp.roll(rim_rows, -1, axis=0), rim_rows)
    before_rim = jnp.where(((block == 0) & (y == 0))[:, None], 0, before_rim)
    after_rim = jnp.where(y == pair - 1, jnp.roll(rim_rows, 1, axis=0), rim_rows)
    after_rim = jnp.where(((block == outer - 1) & (y == pair - 1))[:, None], 0, after_rim)
    sub = lax.rem(x + jnp.arange(inner), inner)[None, :, None]
    before_low = jnp.where(sub == 0, before_rim[:, None], jnp.roll(across[1], 1, axis=1))
    after_high = jnp.where(sub == inner - 1, after_rim[:, None], jnp.roll(across[0], -1, axis=1))
    before = jnp.where(c == 0, before_low, across[1])
    after = jnp.where(c == 0, across[0], after_high)
    return before.reshape(outer * inner, -1), after.reshape(outer * inner, -1)


def spread_body(
    mixer_input,
    time_step,
    damping,
    input_map,
    readout,
    skip_gain,
    out_gain,
    out_weight,
    residual,
    channel_gain,
    value_weight,
    gate_weight,
    value_taps,
    gate_taps,
    down_weight,
):
    tp_count, sp_count = lax.axis_size("tp"), lax.axis_size("sp")
    outer, inner = sp_count // pair, tp_count // pair
    tok_rows, local_width = mixer_input.shape
    own_rows = tok_rows // tp_count
    model = residual.shape[1]
    z, tp = lax.axis_index("sp") // pair, lax.axis_index("tp")

    def columns(weight):
        return jnp.swapaxes(weight.reshape(weight.shape[0], outer, -1), 0, 1)

    value_stacks = spread(columns(value_weight))
    scal, xt, yt, rows_a, ends = mixer_local(mixer_input, time_step, damping, input_map, readout)
    every = lax.all_to_all(
        jnp.broadcast_to(ends[None], (sp_count,) + ends.shape), "sp", 0, 0, tiled=True
    )
    gate_stacks = spread(columns(gate_weight))
    others = outer_send(lambda s: residual, "tp", pair)
    taps = jnp.stack((value_taps, gate_taps), axis=1).reshape(-1, value_taps.shape[1])
    taps = lax.dynamic_index_in_dim(taps.reshape(taps.shape[0], outer, -1), z, 1, False)
    taps_over = lax.ppermute(taps, "tp", ring("tp", pair, 0, 1))
    taps = jnp.stack((taps, taps_over), axis=1).reshape(value_taps.shape[0], -1)

    mixed = mixer_carried(scal, xt, yt, rows_a, every, readout, skip_gain, out_gain)
    mixed = lax.all_gather(mixed, "tp", axis=0)
    squares = jnp.sum(mixed[:, local_width:].astype(f32), axis=(0, 1))
    inverse = lax.rsqrt(squares / (local_width * tp_count) + norm_eps)
    channels = mixed[:, :local_width].reshape(local_width * tp_count, tok_rows)
    mixed_rows = (
        lax.dot_general(channels, out_weight, (((0,), (0,)), ((), ())), preferred_element_type=f32)
        * inverse[:, None]
    )
    picked = [
        lax.dynamic_slice_in_dim(
            mixed_rows, lax.rem(tp + tp_count - pair * r, tp_count) * own_rows, own_rows, axis=0
        )
        for r in range(inner)
    ]
    order = [0] + list(range(inner - 1, 0, -1))
    picked = jnp.concatenate([picked[r] for r in order], axis=0)
    mine = [residual] + others
    rows = jnp.concatenate([mine[r] for r in order], axis=0)
    hidden_state = (rows.astype(f32) + picked).astype(bf16)
    state_wide = hidden_state.astype(f32)
    scale_rows = lax.rsqrt(jnp.mean(state_wide * state_wide, axis=1, keepdims=True) + norm_eps)
    normed = (state_wide * scale_rows * channel_gain[None, :]).astype(bf16)
    x_rows = jnp.concatenate([normed] + outer_send(lambda s: normed, "sp", pair), axis=0)
    up = up_projection(x_rows, value_stacks + gate_stacks)
    down_stacks = spread(down_weight.reshape(outer, -1, down_weight.shape[1]))
    before, after = edges_of(up, outer, inner)
    partial = down_projection(up, before, after, taps, down_stacks)
    parts = partial.reshape(outer, inner, own_rows, model)
    total = parts[:, 0].astype(f32)
    for got in outer_send(lambda s: parts[:, s], "tp", pair):
        total = total + got.astype(f32)
    total = total.astype(bf16)
    summed = total[0].astype(f32)
    for got in outer_send(lambda s: total[outer - s], "sp", pair):
        summed = summed + got.astype(f32)
    return (state_wide[:own_rows] + summed).astype(bf16)


def solution(mesh):
    in_specs = (
        P("sp", "tp"),
        P(None, "tp"),
        P(None, "sp", "tp"),
        P(None, None, "tp", None, None),
        P(None, None, "tp", None, None),
        P("tp"),
        P("tp"),
        P(),
        P(("sp", "tp"), None),
        P(),
        P("sp", "tp"),
        P("sp", "tp"),
        P(None, "tp"),
        P(None, "tp"),
        P("tp", "sp"),
    )
    out_specs = P(("sp", "tp"), None)

    def body(*args):
        value_weight = args[10]
        sp, tp = mesh.shape["sp"], mesh.shape["tp"]
        even = sp % pair == 0 and tp % pair == 0
        whole_lanes = even and (value_weight.shape[1] // (sp // pair)) % 128 == 0
        return (spread_body if whole_lanes else gathered_body)(*args)

    return jax.shard_map(body, mesh=mesh, in_specs=in_specs, out_specs=out_specs, check_vma=False)
```

```python
import math

import jax
import jax.numpy as jnp
from jax import lax
from jax.experimental import pallas as pl
from jax.experimental.pallas import tpu as pltpu
from jax.sharding import PartitionSpec as P


norm_eps = 1e-06
highest = lax.Precision.HIGHEST
f32 = jnp.float32
bf16 = jnp.bfloat16


def split2(a):
    top = a.astype(bf16)
    return top, (a - top.astype(f32)).astype(bf16)


def dot3(a, b):
    a0, a1 = split2(a)
    b0, b1 = split2(b)
    total = jnp.dot(a0, b0, preferred_element_type=f32)
    total += jnp.dot(a0, b1, preferred_element_type=f32)
    return total + jnp.dot(a1, b0, preferred_element_type=f32)


def over_rows(a, b):
    return lax.dot_general(a, b, (((0,), (0,)), ((), ())), preferred_element_type=f32)


def cos_sin(coarse, fine, count):
    first = coarse * count
    first = first - jnp.floor(first + 0.5)
    turn = first + fine * count
    half = jnp.floor(2.0 * turn + 0.5)
    angle = (2.0 * math.pi) * (turn - 0.5 * half)
    odd = half - 2.0 * jnp.floor(0.5 * half)
    sign = 1.0 - 2.0 * odd
    z = angle * angle
    sine = jnp.full_like(z, -1.0 / 39916800.0)
    for c in (1.0 / 362880.0, -1.0 / 5040.0, 1.0 / 120.0, -1.0 / 6.0, 1.0):
        sine = sine * z + c
    cosine = jnp.full_like(z, 1.0 / 479001600.0)
    for c in (-1.0 / 3628800.0, 1.0 / 40320.0, -1.0 / 720.0, 1.0 / 24.0, -0.5, 1.0):
        cosine = cosine * z + c
    return cosine * sign, sine * (angle * sign)


def iota(shape, dim):
    return lax.broadcasted_iota(jnp.int32, shape, dim)


def turns_of(states, rows, backward):
    when = iota((states, rows), 1)
    when = rows - 1 - when if backward else when
    return (iota((states, rows), 0) * when).astype(f32)


def local_kernel(scal, half_step, xt, damp, in_map, readout, yt, ends, rows_a):
    groups, rows = damp.shape[1], damp.shape[2]
    chans, states = in_map.shape[3], in_map.shape[4]
    part, quarter = states // 2, 2 * groups
    lane = iota((part, ends.shape[2]), 1)
    slim = iota((8, ends.shape[2]), 1)
    row_id, col_id = iota((rows, rows), 0), iota((rows, rows), 1)
    kept = (row_id <= col_id, row_id >= col_id)
    for k in range(2):
        steps = damp[k] + half_step[k]
        rows_a[k] = jnp.dot(steps, kept[k].astype(f32), precision=highest)
    counts = [turns_of(states, rows, k == 1) for k in range(2)]

    def group(g, carry):
        held, spans = carry
        at = pl.ds(pl.multiple_of(g * chans, chans), chans)
        x = xt[at, :]
        total = jnp.zeros((chans, rows), f32)
        for k in range(2):
            cosine, sine = cos_sin(scal[0, k, g], scal[1, k, g], counts[k])
            scale = scal[2, k, g]
            drive_r = over_rows(in_map[k, 0, g], x) * scale
            drive_i = over_rows(in_map[k, 1, g], x) * scale
            turned = jnp.concatenate(
                (cosine * drive_r + sine * drive_i, cosine * drive_i - sine * drive_r), axis=0
            )
            across = jnp.broadcast_to(rows_a[k, pl.ds(g, 1), :], (rows, rows))
            decay = jnp.exp(jnp.where(kept[k], across.T - across, -1e30))
            z = dot3(turned, decay)
            z_r, z_i = z[:states], z[states:]
            s_r = cosine * z_r - sine * z_i
            s_i = cosine * z_i + sine * z_r
            total += dot3(readout[k, 0, g], s_r) - dot3(readout[k, 1, g], s_i)
            last = 0 if k else rows - 1
            spans = jnp.where(slim == k * groups + g, across[:8, last : last + 1], spans)
            for p, s in enumerate((s_r, s_i)):
                col = s[:, last : last + 1]
                for half in range(2):
                    spot = (half * 2 + p) * quarter + k * groups + g
                    held = jnp.where(lane == spot, col[half * part : (half + 1) * part], held)
        yt[at, :] = total
        return held, spans

    start = (jnp.zeros(lane.shape, f32), jnp.zeros(slim.shape, f32))
    held, spans = lax.fori_loop(0, groups, group, start, unroll=4)
    for peer in range(ends.shape[0]):
        ends[peer, :part] = held
        ends[peer, part:] = spans


def carry_kernel(scal, place, xt, rows_a, lanes, every, readout, yt, skip, gain, out):
    groups, rows = rows_a.shape[1], rows_a.shape[2]
    chans, states = readout.shape[3], readout.shape[4]
    blocks = every.shape[0]
    part, quarter = states // 2, 2 * groups
    mine = place[0]
    number = iota((states, quarter), 0).astype(f32)
    backward = iota((states, quarter), 1) >= groups
    coarse, fine = lanes[0:1, :], lanes[1:2, :]
    far_r, far_i = cos_sin(coarse, fine, number * rows)
    near_r, near_i = cos_sin(coarse, fine, number)

    def piece(b, p):
        ref = every.at[b]
        return jnp.concatenate(
            [ref[:part, (h * 2 + p) * quarter : (h * 2 + p + 1) * quarter] for h in range(2)], axis=0
        )

    c_r = jnp.zeros((states, quarter), f32)
    c_i = jnp.zeros((states, quarter), f32)
    for b in range(blocks - 1):
        other = blocks - 1 - b
        e_r = jnp.where(backward, piece(other, 0), piece(b, 0))
        e_i = jnp.where(backward, piece(other, 1), piece(b, 1))
        span = jnp.where(
            backward[:1], every[other, part : part + 1, :quarter], every[b, part : part + 1, :quarter]
        )
        fade = jnp.exp(-span)
        n_r = fade * (far_r * c_r - far_i * c_i) + e_r
        n_i = fade * (far_r * c_i + far_i * c_r) + e_i
        place_in = jnp.where(backward, blocks - 1 - mine, mine)
        c_r = jnp.where(b < place_in, n_r, c_r)
        c_i = jnp.where(b < place_in, n_i, c_i)
    w_r = near_r * c_r - near_i * c_i
    w_i = near_r * c_i + near_i * c_r
    counts = [turns_of(states, rows, k == 1) for k in range(2)]
    squares = jnp.zeros((8, rows), f32)
    for g in range(groups):
        at = pl.ds(g * chans, chans)
        total = yt[at, :] + skip[at, :] * xt[at, :].astype(f32)
        for k in range(2):
            cosine, sine = cos_sin(scal[0, k, g], scal[1, k, g], counts[k])
            l = k * groups + g
            a, b = w_r[:, l : l + 1], w_i[:, l : l + 1]
            fade = jnp.exp(-rows_a[k, g : g + 1, :])
            s_r = (cosine * a - sine * b) * fade
            s_i = (cosine * b + sine * a) * fade
            total += dot3(readout[k, 0, g], s_r) - dot3(readout[k, 1, g], s_i)
        for r in range(0, chans, 8):
            squares += total[r : r + 8] * total[r : r + 8]
        out[at, :] = (total * gain[at, :]).astype(bf16)
    square = jnp.sum(squares, axis=0, keepdims=True)
    top = square.astype(bf16)
    rest = square - top.astype(f32)
    mid = rest.astype(bf16)
    low = (rest - mid.astype(f32)).astype(bf16)
    extra = out.shape[0] - groups * chans
    which = iota((extra, rows), 0)
    tail = jnp.where(which == 0, top.astype(f32), jnp.where(which == 1, mid.astype(f32), low.astype(f32)))
    tail = jnp.where(which < 3, tail, 0.0)
    out[pl.ds(groups * chans, extra), :] = tail.astype(bf16)


square_rows = 16


def vmem(count):
    return [pl.BlockSpec(memory_space=pltpu.VMEM)] * count


def mixer_local(mixer_input, time_step, damping, input_map, readout):
    rows, width = mixer_input.shape
    groups = time_step.shape[1]
    states = input_map.shape[3]
    half_step = 0.5 * time_step
    coarse = jnp.floor(half_step * 2048.0) / 2048.0
    scal = jnp.stack((coarse, half_step - coarse, jnp.sqrt(-jnp.expm1(-time_step))))
    damp = jnp.swapaxes(damping, 1, 2)
    xt = mixer_input.T
    lanes = 8 * groups
    smem = pl.BlockSpec(memory_space=pltpu.SMEM)
    yt, ends, rows_a = pl.pallas_call(
        local_kernel,
        out_shape=(
            jax.ShapeDtypeStruct((width, rows), f32),
            jax.ShapeDtypeStruct((lax.axis_size("sp"), states // 2 + 8, lanes), f32),
            jax.ShapeDtypeStruct(damp.shape, f32),
        ),
        in_specs=[smem] + vmem(5),
        out_specs=tuple(vmem(3)),
        name="mixer_local",
    )(scal, half_step[:, :, None], xt, damp, jnp.swapaxes(input_map, 3, 4), readout)
    return scal, xt, yt, rows_a, ends


def mixer_carried(scal, xt, yt, rows_a, every, readout, skip_gain, out_gain):
    width, rows = xt.shape
    smem = pl.BlockSpec(memory_space=pltpu.SMEM)
    place = lax.axis_index("sp").reshape(1)
    lanes = scal[:2].reshape(2, -1)
    return pl.pallas_call(
        carry_kernel,
        out_shape=jax.ShapeDtypeStruct((width + square_rows, rows), bf16),
        in_specs=[smem, smem] + vmem(8),
        out_specs=pl.BlockSpec(memory_space=pltpu.VMEM),
        name="mixer_carried",
    )(scal, place, xt, rows_a, lanes, every, readout, yt, skip_gain[:, None], out_gain[:, None])


def with_halo(cells, axis):
    count = lax.axis_size(axis)
    return jnp.concatenate(
        [
            lax.ppermute(cells[-1:], axis, [(i, i + 1) for i in range(count - 1)]),
            cells,
            lax.ppermute(cells[:1], axis, [(i + 1, i) for i in range(count - 1)]),
        ],
        axis=0,
    )


def gathered_body(
    mixer_input,
    time_step,
    damping,
    input_map,
    readout,
    skip_gain,
    out_gain,
    out_weight,
    residual,
    channel_gain,
    value_weight,
    gate_weight,
    value_taps,
    gate_taps,
    down_weight,
):
    tp_count = lax.axis_size("tp")
    tok_rows, local_width = mixer_input.shape
    residual_rows = lax.all_gather(residual, "tp", axis=0, tiled=True)
    scal, xt, yt, rows_a, ends = mixer_local(mixer_input, time_step, damping, input_map, readout)
    every = lax.all_to_all(ends, "sp", 0, 0, tiled=True)
    mixed = mixer_carried(scal, xt, yt, rows_a, every, readout, skip_gain, out_gain)
    mixed = lax.all_gather(mixed, "tp", axis=0)
    squares = jnp.sum(mixed[:, local_width:].astype(f32), axis=(0, 1))
    inverse = lax.rsqrt(squares / (local_width * tp_count) + norm_eps)
    channels = mixed[:, :local_width].reshape(local_width * tp_count, tok_rows)
    mixed_rows = (
        lax.dot_general(channels, out_weight, (((0,), (0,)), ((), ())), preferred_element_type=f32)
        * inverse[:, None]
    )
    hidden_state = (residual_rows.astype(f32) + mixed_rows).astype(bf16)
    state_wide = hidden_state.astype(f32)
    scale_rows = lax.rsqrt(jnp.mean(state_wide * state_wide, axis=1, keepdims=True) + norm_eps)
    block_rows = (state_wide * scale_rows * channel_gain[None, :]).astype(bf16)
    hidden_width = value_weight.shape[1]
    value_up = jnp.dot(
        block_rows,
        lax.all_gather(value_weight, "sp", axis=0, tiled=True),
        preferred_element_type=f32,
    )
    gate_up = jnp.dot(
        block_rows,
        lax.all_gather(gate_weight, "sp", axis=0, tiled=True),
        preferred_element_type=f32,
    )
    both_up = jnp.concatenate((value_up.astype(bf16), gate_up.astype(bf16)), axis=1)
    padded = with_halo(both_up, "sp")
    taps = jnp.concatenate((value_taps, gate_taps), axis=1)
    convolved = (
        taps[0] * padded[:-2].astype(f32)
        + taps[1] * padded[1:-1].astype(f32)
        + taps[2] * padded[2:].astype(f32)
    )
    hidden = (convolved[:, :hidden_width] * jax.nn.silu(convolved[:, hidden_width:])).astype(bf16)
    down_full = lax.all_gather(down_weight, "sp", axis=1, tiled=True)
    partial = jnp.dot(hidden, down_full, preferred_element_type=f32).astype(bf16)
    pieces = lax.all_to_all(
        partial.reshape(tp_count, tok_rows // tp_count, -1), "tp", 0, 0, tiled=True
    )
    mine = lax.axis_index("tp") * (tok_rows // tp_count)
    own = lax.dynamic_slice_in_dim(state_wide, mine, tok_rows // tp_count, axis=0)
    return (own + jnp.sum(pieces.astype(f32), axis=0)).astype(bf16)


def ring(axis, inner, step, low=0):
    size = lax.axis_size(axis)
    outer = size // inner
    return [
        (i, ((i // inner + step) % outer) * inner + (i + low) % inner) for i in range(size)
    ]


def outer_send(pick, axis, inner):
    outer = lax.axis_size(axis) // inner
    return [lax.ppermute(pick(s), axis, ring(axis, inner, s)) for s in range(1, outer)]


def cut_of(shapes, outer):
    def call(*weights):
        outs = tuple(
            jax.ShapeDtypeStruct(shape, bf16) for shape in shapes for _ in range(outer)
        )
        hbm = pl.BlockSpec(memory_space=pltpu.HBM)
        pieces = pl.pallas_call(
            cut_all(len(weights)),
            out_shape=outs,
            in_specs=[hbm] * len(weights),
            out_specs=tuple(vmem(len(outs))),
            scratch_shapes=[pltpu.SemaphoreType.DMA((len(outs),))],
            name="cut_weights",
        )(*weights)
        return [pieces[k * outer : (k + 1) * outer] for k in range(len(weights))]

    return call


def cut_all(count):
    def kernel(*refs):
        ins, outs, sems = refs[:count], refs[count:-1], refs[-1]
        outer = len(outs) // count
        mine = lax.axis_index("sp") // pair
        copies = []
        for w in range(count):
            for s in range(outer):
                out = outs[w * outer + s]
                rows, cols = out.shape
                there = lax.rem(mine + s, outer)
                if rows == ins[w].shape[0]:
                    part = ins[w].at[:, pl.ds(pl.multiple_of(there * cols, cols), cols)]
                else:
                    part = ins[w].at[pl.ds(pl.multiple_of(there * rows, rows), rows), :]
                copy = pltpu.make_async_copy(part, out, sems.at[w * outer + s])
                copy.start()
                copies.append(copy)
        for copy in copies:
            copy.wait()

    return kernel


def spread(pieces):
    moved = outer_send(lambda s: pieces[s], "sp", pair)
    own = jnp.stack([pieces[0]] + moved)
    beside = lax.ppermute(own, "sp", ring("sp", pair, 0, 1))
    over = ring("tp", pair, 0, 1)
    across = lax.ppermute(own, "tp", over)
    return own, beside, across, lax.ppermute(beside, "tp", over)


pair = 2


def row_block(outer, which, step):
    sp = lax.axis_index("sp")
    far = lax.rem(sp // pair + outer - step, outer)
    return far * pair + lax.rem(sp + which, pair)


def up_kernel(*refs):
    stacks, (out, edges, x, last, full, sems) = refs[:8], refs[-6:]
    rows_in = refs[8:-6]
    outer, rows, cols = stacks[0].shape
    groups = []
    for kind in range(2):
        copies = []
        for core in range(2):
            for which in range(2):
                ref = stacks[kind * 4 + core * 2 + which]
                for s in range(outer):
                    first = pl.multiple_of(row_block(outer, which, s) * rows, rows)
                    copy = pltpu.make_async_copy(
                        ref.at[s],
                        full.at[kind, pl.ds(first, rows), pl.ds(core * cols, cols)],
                        sems.at[kind * 2 + core, which * outer + s],
                    )
                    copy.start()
                    copies.append(copy)
        groups.append(copies)
    each = rows_in[0].shape[0]
    for s, ref in enumerate(rows_in):
        x[s * each : (s + 1) * each, :] = ref[...]
    pieces = edges.shape[1]
    for kind, copies in enumerate(groups):
        for copy in copies:
            copy.wait()
        part = jnp.dot(x[...], full[kind], preferred_element_type=f32)
        first = 2 * kind * cols
        out[:, first : first + 2 * cols] = part.astype(bf16)
        length = part.shape[0] // pieces
        for p in range(pieces):
            for end, at in ((0, p * length), (1, (p + 1) * length - 1)):
                row = part[at : at + 1]
                last[end, p : p + 1, first : first + cols] = row[:, cols:]
                last[end, p : p + 1, first + cols : first + 2 * cols] = row[:, :cols]
    edges[...] = last[...].astype(bf16)


def down_kernel(up, before, after, taps, *refs):
    stacks, outs, (full, sems) = refs[:4], refs[4:-2], refs[-2:]
    outer, rows, cols = stacks[0].shape
    copies = []
    for core in range(2):
        for which in range(2):
            ref = stacks[core * 2 + which]
            for s in range(outer):
                first = pl.multiple_of(row_block(outer, which, s) * cols, cols)
                copy = pltpu.make_async_copy(
                    ref.at[s],
                    full.at[pl.ds(core * rows, rows), pl.ds(first, cols)],
                    sems.at[core * 2 + which, s],
                )
                copy.start()
                copies.append(copy)
    width = 2 * rows
    count, pieces = up.shape[0], before.shape[0]
    length = count // pieces

    def convolved(start):
        at = slice(start, start + width)
        rows_id = iota((length, width), 0)
        done = []
        for p in range(pieces):
            cells = up[p * length : (p + 1) * length, at].astype(f32)
            left = pltpu.roll(cells, 1, 0)
            left = jnp.where(rows_id == 0, before[p : p + 1, at].astype(f32), left)
            right = pltpu.roll(cells, length - 1, 0)
            right = jnp.where(rows_id == length - 1, after[p : p + 1, at].astype(f32), right)
            done.append(taps[0:1, at] * left + taps[1:2, at] * cells + taps[2:3, at] * right)
        return jnp.concatenate(done, axis=0)

    gate = convolved(width)
    hidden = (convolved(0) * (gate / (1.0 + jnp.exp(-gate)))).astype(bf16)
    for copy in copies:
        copy.wait()
    partial = jnp.dot(hidden, full[...], preferred_element_type=f32).astype(bf16)
    for p in range(pieces):
        outs[p % len(outs)][p // len(outs)] = partial[p * length : (p + 1) * length]


def up_projection(rows_in, stacks, pieces):
    outer, rows, cols = stacks[0].shape
    count = sum(r.shape[0] for r in rows_in)
    return pl.pallas_call(
        up_kernel,
        out_shape=(
            jax.ShapeDtypeStruct((count, 4 * cols), bf16),
            jax.ShapeDtypeStruct((2, pieces, 4 * cols), bf16),
        ),
        in_specs=[pl.BlockSpec(memory_space=pltpu.HBM)] * 8 + vmem(len(rows_in)),
        out_specs=tuple(vmem(2)),
        scratch_shapes=[
            pltpu.VMEM((count, rows_in[0].shape[1]), bf16),
            pltpu.VMEM((2, pieces, 4 * cols), f32),
            pltpu.VMEM((2, 2 * outer * rows, 2 * cols), bf16),
            pltpu.SemaphoreType.DMA((4, 2 * outer)),
        ],
        name="up_projection",
    )(*stacks, *rows_in)


def down_projection(up, before, after, taps, stacks, inner):
    outer, rows, cols = stacks[0].shape
    return pl.pallas_call(
        down_kernel,
        out_shape=(
            jax.ShapeDtypeStruct(
                (outer, up.shape[0] // (outer * inner), 2 * outer * cols), bf16
            ),
        )
        * inner,
        in_specs=vmem(4) + [pl.BlockSpec(memory_space=pltpu.HBM)] * 4,
        out_specs=tuple(vmem(inner)),
        scratch_shapes=[
            pltpu.VMEM((2 * rows, 2 * outer * cols), bf16),
            pltpu.SemaphoreType.DMA((4, outer)),
        ],
        name="down_projection",
    )(up, before, after, taps, *stacks)


def edges_of(ends, outer, inner):
    sp, tp = lax.axis_index("sp"), lax.axis_index("tp")
    z, y, x, c = sp // pair, lax.rem(sp, pair), tp // pair, lax.rem(tp, pair)
    ends = ends.reshape(2, outer, inner, -1)
    across = lax.ppermute(ends, "tp", ring("tp", pair, 0, 1))
    rim = jnp.where(c == 0, lax.rem(inner - x, inner), inner - 1 - x)
    out_edge = lax.dynamic_index_in_dim(
        lax.dynamic_index_in_dim(ends, c, 0, False), rim, 1, False
    )
    sizes = (lax.axis_size("sp"), lax.axis_size("tp"))
    hops = [
        (i * sizes[1] + j, (i ^ 1) * sizes[1] + (j ^ 1))
        for i in range(sizes[0])
        for j in range(sizes[1])
    ]
    rim_rows = lax.ppermute(out_edge, ("sp", "tp"), hops)
    block = lax.rem(z + outer - jnp.arange(outer), outer)
    before_rim = jnp.where(y == 0, jnp.roll(rim_rows, -1, axis=0), rim_rows)
    before_rim = jnp.where(((block == 0) & (y == 0))[:, None], 0, before_rim)
    after_rim = jnp.where(y == pair - 1, jnp.roll(rim_rows, 1, axis=0), rim_rows)
    after_rim = jnp.where(((block == outer - 1) & (y == pair - 1))[:, None], 0, after_rim)
    sub = lax.rem(x + jnp.arange(inner), inner)[None, :, None]
    before_low = jnp.where(sub == 0, before_rim[:, None], jnp.roll(across[1], 1, axis=1))
    after_high = jnp.where(sub == inner - 1, after_rim[:, None], jnp.roll(across[0], -1, axis=1))
    before = jnp.where(c == 0, before_low, across[1])
    after = jnp.where(c == 0, across[0], after_high)
    return before.reshape(outer * inner, -1), after.reshape(outer * inner, -1)


def spread_body(
    mixer_input,
    time_step,
    damping,
    input_map,
    readout,
    skip_gain,
    out_gain,
    out_weight,
    residual,
    channel_gain,
    value_weight,
    gate_weight,
    value_taps,
    gate_taps,
    down_weight,
):
    tp_count, sp_count = lax.axis_size("tp"), lax.axis_size("sp")
    outer, inner = sp_count // pair, tp_count // pair
    tok_rows, local_width = mixer_input.shape
    own_rows = tok_rows // tp_count
    z, tp = lax.axis_index("sp") // pair, lax.axis_index("tp")

    wide = (value_weight.shape[0], value_weight.shape[1] // outer)
    deep = (down_weight.shape[0] // outer, down_weight.shape[1])
    (value_pieces,) = cut_of((wide,), outer)(value_weight)
    gate_pieces, down_pieces = cut_of((wide, deep), outer)(gate_weight, down_weight)
    value_stacks = spread(value_pieces)
    scal, xt, yt, rows_a, ends = mixer_local(mixer_input, time_step, damping, input_map, readout)
    every = lax.all_to_all(ends, "sp", 0, 0, tiled=True)
    gate_stacks = spread(gate_pieces)
    others = outer_send(lambda s: residual, "tp", pair)
    taps = jnp.stack((value_taps, gate_taps), axis=1).reshape(-1, value_taps.shape[1])
    taps = lax.dynamic_index_in_dim(taps.reshape(taps.shape[0], outer, -1), z, 1, False)
    taps_over = lax.ppermute(taps, "tp", ring("tp", pair, 0, 1))
    taps = jnp.stack((taps, taps_over), axis=1).reshape(value_taps.shape[0], -1)

    mixed = mixer_carried(scal, xt, yt, rows_a, every, readout, skip_gain, out_gain)
    mixed = lax.all_gather(mixed, "tp", axis=0)
    squares = jnp.sum(mixed[:, local_width:].astype(f32), axis=(0, 1))
    inverse = lax.rsqrt(squares / (local_width * tp_count) + norm_eps)
    channels = mixed[:, :local_width].reshape(local_width * tp_count, tok_rows)
    mixed_rows = (
        lax.dot_general(channels, out_weight, (((0,), (0,)), ((), ())), preferred_element_type=f32)
        * inverse[:, None]
    )
    picked = [
        lax.dynamic_slice_in_dim(
            mixed_rows, lax.rem(tp + tp_count - pair * r, tp_count) * own_rows, own_rows, axis=0
        )
        for r in range(inner)
    ]
    order = [0] + list(range(inner - 1, 0, -1))
    picked = jnp.concatenate([picked[r] for r in order], axis=0)
    mine = [residual] + others
    rows = jnp.concatenate([mine[r] for r in order], axis=0)
    hidden_state = (rows.astype(f32) + picked).astype(bf16)
    state_wide = hidden_state.astype(f32)
    scale_rows = lax.rsqrt(jnp.mean(state_wide * state_wide, axis=1, keepdims=True) + norm_eps)
    normed = (state_wide * scale_rows * channel_gain[None, :]).astype(bf16)
    moved = outer_send(lambda s: normed, "sp", pair)
    up, ends = up_projection([normed] + moved, value_stacks + gate_stacks, outer * inner)
    down_stacks = spread(down_pieces)
    before, after = edges_of(ends, outer, inner)
    parts = down_projection(up, before, after, taps, down_stacks, inner)
    total = parts[0].astype(f32)
    for got in outer_send(lambda s: parts[s], "tp", pair):
        total = total + got.astype(f32)
    total = total.astype(bf16)
    summed = total[0].astype(f32)
    for got in outer_send(lambda s: total[outer - s], "sp", pair):
        summed = summed + got.astype(f32)
    return (state_wide[:own_rows] + summed).astype(bf16)


def solution(mesh):
    in_specs = (
        P("sp", "tp"),
        P(None, "tp"),
        P(None, "sp", "tp"),
        P(None, None, "tp", None, None),
        P(None, None, "tp", None, None),
        P("tp"),
        P("tp"),
        P(),
        P(("sp", "tp"), None),
        P(),
        P("sp", "tp"),
        P("sp", "tp"),
        P(None, "tp"),
        P(None, "tp"),
        P("tp", "sp"),
    )
    out_specs = P(("sp", "tp"), None)

    def body(*args):
        value_weight = args[10]
        sp, tp = mesh.shape["sp"], mesh.shape["tp"]
        even = sp % pair == 0 and tp % pair == 0
        whole_lanes = even and (value_weight.shape[1] // (sp // pair)) % 128 == 0
        if not whole_lanes:
            return gathered_body(*args)
        return spread_body(*args)

    return jax.shard_map(body, mesh=mesh, in_specs=in_specs, out_specs=out_specs, check_vma=False)
```

```python
import functools
import math

import jax
import jax.numpy as jnp
from jax import lax
from jax.experimental import pallas as pl
from jax.experimental.pallas import tpu as pltpu
from jax.sharding import PartitionSpec as P


norm_eps = 1e-06
f32 = jnp.float32
bf16 = jnp.bfloat16


def split2(a):
    top = a.astype(bf16)
    return top, (a - top.astype(f32)).astype(bf16)


def dot3(a, b):
    rows = a.shape[0]
    a0, a1 = split2(a)
    b0, b1 = split2(b)
    both = jnp.dot(jnp.concatenate((a0, a1), axis=0), b0, preferred_element_type=f32)
    return both[:rows] + both[rows:] + jnp.dot(a0, b1, preferred_element_type=f32)


def four_wide(ref, g):
    return jnp.concatenate([ref[k, p, g] for k in range(2) for p in range(2)], axis=1)


def signed_wide(readout, g):
    parts = [readout[k, p, g] for k in range(2) for p in range(2)]
    return jnp.concatenate((parts[0], -parts[1], parts[2], -parts[3]), axis=1)


def over_rows(a, b):
    return lax.dot_general(a, b, (((0,), (0,)), ((), ())), preferred_element_type=f32)


def cos_sin(coarse, fine, count):
    first = coarse * count
    first = first - jnp.floor(first + 0.5)
    turn = first + fine * count
    half = jnp.floor(2.0 * turn + 0.5)
    angle = (2.0 * math.pi) * (turn - 0.5 * half)
    odd = half - 2.0 * jnp.floor(0.5 * half)
    sign = 1.0 - 2.0 * odd
    z = angle * angle
    sine = jnp.full_like(z, -1.0 / 39916800.0)
    for c in (1.0 / 362880.0, -1.0 / 5040.0, 1.0 / 120.0, -1.0 / 6.0, 1.0):
        sine = sine * z + c
    cosine = jnp.full_like(z, 1.0 / 479001600.0)
    for c in (-1.0 / 3628800.0, 1.0 / 40320.0, -1.0 / 720.0, 1.0 / 24.0, -0.5, 1.0):
        cosine = cosine * z + c
    return cosine * sign, sine * (angle * sign)


def iota(shape, dim):
    return lax.broadcasted_iota(jnp.int32, shape, dim)


def turns_of(states, rows, backward):
    when = iota((states, rows), 1)
    when = rows - 1 - when if backward else when
    return (iota((states, rows), 0) * when).astype(f32)


def local_kernel(scal, x_in, damp, in_map, readout, yt, xt, ends, rows_a):
    groups, rows = damp.shape[1], damp.shape[2]
    chans, states = in_map.shape[3], in_map.shape[4]
    part, quarter = states // 2, 2 * groups
    lane = iota((part, ends.shape[2]), 1)
    slim = iota((8, ends.shape[2]), 1)
    row_id, col_id = iota((rows, rows), 0), iota((rows, rows), 1)
    kept = (row_id <= col_id, row_id >= col_id)
    for k in range(2):
        ones = kept[k].astype(f32).astype(bf16)
        left = damp[k]
        sums = jnp.zeros(left.shape, f32)
        for _ in range(3):
            part_of = left.astype(bf16)
            sums += jnp.dot(part_of, ones, preferred_element_type=f32)
            left = left - part_of.astype(f32)
        rows_a[k] = sums
    xt[...] = x_in[...].astype(f32).T.astype(bf16)
    since = iota((1, rows), 1).astype(f32) + 1.0
    elapsed = (since, rows + 1.0 - since)
    counts = [turns_of(states, rows, k == 1) for k in range(2)]

    def group(g, carry):
        held, spans = carry
        at = pl.ds(pl.multiple_of(g * chans, chans), chans)
        x = xt[at, :]
        drives = over_rows(four_wide(in_map, g), x)
        joined = []
        for k in range(2):
            cosine, sine = cos_sin(scal[0, k, g], scal[1, k, g], counts[k])
            scale = scal[2, k, g]
            drive_r = drives[2 * k * states : (2 * k + 1) * states] * scale
            drive_i = drives[(2 * k + 1) * states : (2 * k + 2) * states] * scale
            turned = jnp.concatenate(
                (cosine * drive_r + sine * drive_i, cosine * drive_i - sine * drive_r), axis=0
            )
            summed = rows_a[k, pl.ds(g, 1), :] + (scal[0, k, g] + scal[1, k, g]) * elapsed[k]
            rows_a[k, pl.ds(g, 1), :] = summed
            across = jnp.broadcast_to(summed, (rows, rows))
            decay = jnp.exp(jnp.where(kept[k], across.T - across, -1e30))
            z = dot3(turned, decay)
            z_r, z_i = z[:states], z[states:]
            s_r = cosine * z_r - sine * z_i
            s_i = cosine * z_i + sine * z_r
            joined += [s_r, s_i]
            last = 0 if k else rows - 1
            spans = jnp.where(slim == k * groups + g, across[:8, last : last + 1], spans)
            for p, s in enumerate((s_r, s_i)):
                col = s[:, last : last + 1]
                for half in range(2):
                    spot = (half * 2 + p) * quarter + k * groups + g
                    held = jnp.where(lane == spot, col[half * part : (half + 1) * part], held)
        yt[at, :] = dot3(signed_wide(readout, g), jnp.concatenate(joined, axis=0))
        return held, spans

    start = (jnp.zeros(lane.shape, f32), jnp.zeros(slim.shape, f32))
    held, spans = lax.fori_loop(0, groups, group, start, unroll=4)
    for peer in range(ends.shape[0]):
        ends[peer, :part] = held
        ends[peer, part:] = spans


def carry_kernel(scal, xt, rows_a, every, readout, yt, skip, gain, out, wide):
    groups, rows = rows_a.shape[1], rows_a.shape[2]
    chans, states = readout.shape[3], readout.shape[4]
    blocks = every.shape[0]
    part, quarter = states // 2, 2 * groups
    mine = lax.axis_index("sp")
    number = iota((states, quarter), 0).astype(f32)
    backward = iota((states, quarter), 1) >= groups
    spot = iota((1, quarter), 1)
    coarse = jnp.zeros((1, quarter), f32)
    fine = jnp.zeros((1, quarter), f32)
    for k in range(2):
        for g in range(groups):
            coarse = jnp.where(spot == k * groups + g, scal[0, k, g], coarse)
            fine = jnp.where(spot == k * groups + g, scal[1, k, g], fine)
    width = skip.shape[1]
    wide[0] = jnp.broadcast_to(skip[...], (rows, width)).T
    wide[1] = jnp.broadcast_to(gain[...], (rows, width)).T
    far_r, far_i = cos_sin(coarse, fine, number * rows)
    near_r, near_i = cos_sin(coarse, fine, number)

    def piece(b, p):
        ref = every.at[b]
        return jnp.concatenate(
            [ref[:part, (h * 2 + p) * quarter : (h * 2 + p + 1) * quarter] for h in range(2)], axis=0
        )

    c_r = jnp.zeros((states, quarter), f32)
    c_i = jnp.zeros((states, quarter), f32)
    for b in range(blocks - 1):
        other = blocks - 1 - b
        e_r = jnp.where(backward, piece(other, 0), piece(b, 0))
        e_i = jnp.where(backward, piece(other, 1), piece(b, 1))
        span = jnp.where(
            backward[:1], every[other, part : part + 1, :quarter], every[b, part : part + 1, :quarter]
        )
        fade = jnp.exp(-span)
        n_r = fade * (far_r * c_r - far_i * c_i) + e_r
        n_i = fade * (far_r * c_i + far_i * c_r) + e_i
        place_in = jnp.where(backward, blocks - 1 - mine, mine)
        c_r = jnp.where(b < place_in, n_r, c_r)
        c_i = jnp.where(b < place_in, n_i, c_i)
    w_r = near_r * c_r - near_i * c_i
    w_i = near_r * c_i + near_i * c_r
    counts = [turns_of(states, rows, k == 1) for k in range(2)]
    squares = jnp.zeros((8, rows), f32)
    for g in range(groups):
        at = pl.ds(g * chans, chans)
        total = yt[at, :] + wide[0, at, :] * xt[at, :].astype(f32)
        joined = []
        for k in range(2):
            cosine, sine = cos_sin(scal[0, k, g], scal[1, k, g], counts[k])
            l = k * groups + g
            a, b = w_r[:, l : l + 1], w_i[:, l : l + 1]
            fade = jnp.exp(-rows_a[k, g : g + 1, :])
            joined += [(cosine * a - sine * b) * fade, (cosine * b + sine * a) * fade]
        total += dot3(signed_wide(readout, g), jnp.concatenate(joined, axis=0))
        for r in range(0, chans, 8):
            squares += total[r : r + 8] * total[r : r + 8]
        out[at, :] = (total * wide[1, at, :]).astype(bf16)
    square = jnp.sum(squares, axis=0, keepdims=True)
    top = square.astype(bf16)
    rest = square - top.astype(f32)
    mid = rest.astype(bf16)
    low = (rest - mid.astype(f32)).astype(bf16)
    extra = out.shape[0] - groups * chans
    which = iota((extra, rows), 0)
    tail = jnp.where(which == 0, top.astype(f32), jnp.where(which == 1, mid.astype(f32), low.astype(f32)))
    tail = jnp.where(which < 3, tail, 0.0)
    out[pl.ds(groups * chans, extra), :] = tail.astype(bf16)


square_rows = 16


def vmem(count):
    return [pl.BlockSpec(memory_space=pltpu.VMEM)] * count


def mixer_local(mixer_input, time_step, damping, input_map, readout):
    rows, width = mixer_input.shape
    groups = time_step.shape[1]
    states = input_map.shape[3]
    half_step = 0.5 * time_step
    coarse = jnp.floor(half_step * 2048.0) / 2048.0
    scal = jnp.stack((coarse, half_step - coarse, jnp.sqrt(-jnp.expm1(-time_step))))
    damp = jnp.swapaxes(damping, 1, 2)
    lanes = 8 * groups
    smem = pl.BlockSpec(memory_space=pltpu.SMEM)
    yt, xt, ends, rows_a = pl.pallas_call(
        local_kernel,
        out_shape=(
            jax.ShapeDtypeStruct((width, rows), f32),
            jax.ShapeDtypeStruct((width, rows), bf16),
            jax.ShapeDtypeStruct((lax.axis_size("sp"), states // 2 + 8, lanes), f32),
            jax.ShapeDtypeStruct(damp.shape, f32),
        ),
        in_specs=[smem] + vmem(4),
        out_specs=tuple(vmem(4)),
        name="mixl",
    )(scal, mixer_input, damp, jnp.swapaxes(input_map, 3, 4), readout)
    return scal, xt, yt, rows_a, ends


def mixer_carried(scal, xt, yt, rows_a, every, readout, skip_gain, out_gain):
    width, rows = xt.shape
    smem = pl.BlockSpec(memory_space=pltpu.SMEM)
    return pl.pallas_call(
        carry_kernel,
        out_shape=jax.ShapeDtypeStruct((width + square_rows, rows), bf16),
        in_specs=[smem] + vmem(7),
        out_specs=pl.BlockSpec(memory_space=pltpu.VMEM),
        scratch_shapes=[pltpu.VMEM((2, width, rows), f32)],
        name="mixc",
    )(scal, xt, rows_a, every, readout, yt, skip_gain[None, :], out_gain[None, :])


def with_halo(cells, axis):
    count = lax.axis_size(axis)
    return jnp.concatenate(
        [
            lax.ppermute(cells[-1:], axis, [(i, i + 1) for i in range(count - 1)]),
            cells,
            lax.ppermute(cells[:1], axis, [(i + 1, i) for i in range(count - 1)]),
        ],
        axis=0,
    )


def gathered_body(
    mixer_input,
    time_step,
    damping,
    input_map,
    readout,
    skip_gain,
    out_gain,
    out_weight,
    residual,
    channel_gain,
    value_weight,
    gate_weight,
    value_taps,
    gate_taps,
    down_weight,
):
    tp_count = lax.axis_size("tp")
    tok_rows, local_width = mixer_input.shape
    residual_rows = lax.all_gather(residual, "tp", axis=0, tiled=True)
    scal, xt, yt, rows_a, ends = mixer_local(mixer_input, time_step, damping, input_map, readout)
    every = lax.all_to_all(ends, "sp", 0, 0, tiled=True)
    mixed = mixer_carried(scal, xt, yt, rows_a, every, readout, skip_gain, out_gain)
    mixed = lax.all_gather(mixed, "tp", axis=0)
    squares = jnp.sum(mixed[:, local_width:].astype(f32), axis=(0, 1))
    inverse = lax.rsqrt(squares / (local_width * tp_count) + norm_eps)
    channels = mixed[:, :local_width].reshape(local_width * tp_count, tok_rows)
    mixed_rows = (
        lax.dot_general(channels, out_weight, (((0,), (0,)), ((), ())), preferred_element_type=f32)
        * inverse[:, None]
    )
    hidden_state = (residual_rows.astype(f32) + mixed_rows).astype(bf16)
    state_wide = hidden_state.astype(f32)
    scale_rows = lax.rsqrt(jnp.mean(state_wide * state_wide, axis=1, keepdims=True) + norm_eps)
    block_rows = (state_wide * scale_rows * channel_gain[None, :]).astype(bf16)
    hidden_width = value_weight.shape[1]
    value_up = jnp.dot(
        block_rows,
        lax.all_gather(value_weight, "sp", axis=0, tiled=True),
        preferred_element_type=f32,
    )
    gate_up = jnp.dot(
        block_rows,
        lax.all_gather(gate_weight, "sp", axis=0, tiled=True),
        preferred_element_type=f32,
    )
    both_up = jnp.concatenate((value_up.astype(bf16), gate_up.astype(bf16)), axis=1)
    padded = with_halo(both_up, "sp")
    taps = jnp.concatenate((value_taps, gate_taps), axis=1)
    convolved = (
        taps[0] * padded[:-2].astype(f32)
        + taps[1] * padded[1:-1].astype(f32)
        + taps[2] * padded[2:].astype(f32)
    )
    hidden = (convolved[:, :hidden_width] * jax.nn.silu(convolved[:, hidden_width:])).astype(bf16)
    down_full = lax.all_gather(down_weight, "sp", axis=1, tiled=True)
    partial = jnp.dot(hidden, down_full, preferred_element_type=f32).astype(bf16)
    pieces = lax.all_to_all(
        partial.reshape(tp_count, tok_rows // tp_count, -1), "tp", 0, 0, tiled=True
    )
    mine = lax.axis_index("tp") * (tok_rows // tp_count)
    own = lax.dynamic_slice_in_dim(state_wide, mine, tok_rows // tp_count, axis=0)
    return (own + jnp.sum(pieces.astype(f32), axis=0)).astype(bf16)


def ring(axis, inner, step, low=0):
    size = lax.axis_size(axis)
    outer = size // inner
    return [
        (i, ((i // inner + step) % outer) * inner + (i + low) % inner) for i in range(size)
    ]


def outer_send(pick, axis, inner):
    outer = lax.axis_size(axis) // inner
    return [lax.ppermute(pick(s), axis, ring(axis, inner, s)) for s in range(1, outer)]


def cut_weights(weights, outer):
    def shape_of(weight):
        rows, cols = weight.shape
        return (rows // outer, cols) if rows > cols else (rows, cols // outer)

    def kernel(*refs):
        ins, outs, sems = refs[: len(weights)], refs[len(weights) : -1], refs[-1]
        mine = lax.axis_index("sp") // pair
        copies = []
        for w, ref in enumerate(ins):
            for s in range(outer):
                there = lax.rem(mine + s, outer)
                out = outs[w * outer + s]
                rows, cols = out.shape
                if rows == ref.shape[0]:
                    part = ref.at[:, pl.ds(pl.multiple_of(there * cols, cols), cols)]
                else:
                    part = ref.at[pl.ds(pl.multiple_of(there * rows, rows), rows), :]
                copy = pltpu.make_async_copy(part, out, sems.at[w, s])
                copy.start()
                copies.append(copy)
        for copy in copies:
            copy.wait()

    outs = tuple(
        jax.ShapeDtypeStruct(shape_of(weight), bf16) for weight in weights for _ in range(outer)
    )
    pieces = pl.pallas_call(
        kernel,
        out_shape=outs,
        in_specs=[pl.BlockSpec(memory_space=pltpu.HBM)] * len(weights),
        out_specs=tuple(vmem(len(outs))),
        scratch_shapes=[pltpu.SemaphoreType.DMA((len(weights), outer))],
        name="cutk",
    )(*weights)
    return [pieces[w * outer : (w + 1) * outer] for w in range(len(weights))]


def spread_pieces(pieces):
    outer = len(pieces)
    own = [pieces[0]]
    for s in range(1, outer):
        own.append(lax.ppermute(pieces[s], "sp", ring("sp", pair, s)))
    beside = []
    for s in range(outer):
        beside.append(lax.ppermute(own[s], "sp", ring("sp", pair, 0, 1)))
    over = ring("tp", pair, 0, 1)
    across = []
    for piece in own + beside:
        across.append(lax.ppermute(piece, "tp", over))
    return own + beside + across


def spread(pieces):
    moved = outer_send(lambda s: pieces[s], "sp", pair)
    own = jnp.stack([pieces[0]] + moved)
    beside = lax.ppermute(own, "sp", ring("sp", pair, 0, 1))
    over = ring("tp", pair, 0, 1)
    across = lax.ppermute(own, "tp", over)
    return own, beside, across, lax.ppermute(beside, "tp", over)


pair = 2


def row_block(outer, which, step):
    sp = lax.axis_index("sp")
    far = lax.rem(sp // pair + outer - step, outer)
    return far * pair + lax.rem(sp + which, pair)


def up_kernel(*refs):
    stacks, (out, edges, rim, x, last, full, sems, row_sems) = refs[:8], refs[-8:]
    rows_in = refs[8:-8]
    outer, rows, cols = stacks[0].shape
    at, row_copies = 0, []
    for n, ref in enumerate(rows_in):
        size = ref.shape[0]
        copy = pltpu.make_async_copy(ref, x.at[at : at + size, :], row_sems.at[n])
        copy.start()
        row_copies.append(copy)
        at += size
    groups = []
    for kind in range(2):
        copies = []
        for core in range(2):
            for which in range(2):
                ref = stacks[kind * 4 + core * 2 + which]
                for s in range(outer):
                    first = pl.multiple_of(row_block(outer, which, s) * rows, rows)
                    copy = pltpu.make_async_copy(
                        ref.at[s],
                        full.at[kind, pl.ds(first, rows), pl.ds(core * cols, cols)],
                        sems.at[kind * 2 + core, which * outer + s],
                    )
                    copy.start()
                    copies.append(copy)
        groups.append(copies)
    for copy in row_copies:
        copy.wait()
    pieces = edges.shape[1]
    for kind, copies in enumerate(groups):
        for copy in copies:
            copy.wait()
        part = jnp.dot(x[...], full[kind], preferred_element_type=f32)
        first = 2 * kind * cols
        out[:, first : first + 2 * cols] = part.astype(bf16)
        length = part.shape[0] // pieces
        for p in range(pieces):
            for end, at in ((0, p * length), (1, (p + 1) * length - 1)):
                row = part[at : at + 1]
                last[end, p : p + 1, first : first + cols] = row[:, cols:]
                last[end, p : p + 1, first + cols : first + 2 * cols] = row[:, :cols]
    edges[...] = last[...].astype(bf16)
    tp = lax.axis_index("tp")
    x_at, c_at = tp // pair, lax.rem(tp, pair)
    inner = pieces // outer
    for s in range(outer):
        row = jnp.zeros((1, last.shape[2]), f32)
        for r in range(inner):
            sub = lax.rem(x_at + r, inner)
            low = last[0, s * inner + r : s * inner + r + 1, :]
            high = last[1, s * inner + r : s * inner + r + 1, :]
            row = jnp.where((c_at == 0) & (sub == 0), low, row)
            row = jnp.where((c_at == 1) & (sub == inner - 1), high, row)
        last[0, s : s + 1, :] = row
    rim[...] = last[0, :outer, :].astype(bf16)


def load_down(held, outer, full, sems):
    rows, cols = held[0].shape
    y = lax.rem(lax.axis_index("sp"), pair)
    copies = []
    for core in range(2):
        for s in range(outer):
            far = lax.rem(lax.axis_index("sp") // pair + outer - s, outer)
            first = pl.multiple_of(far * cols, cols)
            for which in range(2):
                n = (core * 2 + which) * outer + s
                into = lax.rem(y + which, pair)
                copy = pltpu.make_async_copy(
                    held[n],
                    full.at[into, pl.ds(core * rows, rows), pl.ds(first, cols)],
                    sems.at[n],
                )
                copy.start()
                copies.append(copy)
    return copies


def down_kernel(outer, up, across, beyond, taps, taps_over, *refs):
    held, outs, (full, sems) = refs[: 4 * outer], refs[4 * outer : -2], refs[-2:]
    copies = load_down(held, outer, full, sems)
    rows = held[0].shape[0]
    width = 2 * rows
    count, pieces = up.shape[0], across.shape[1]
    length, inner = count // pieces, pieces // outer
    sp, tp = lax.axis_index("sp"), lax.axis_index("tp")
    z, y, x, c = sp // pair, lax.rem(sp, pair), tp // pair, lax.rem(tp, pair)

    def convolved(start):
        at = slice(start, start + width)
        low, high = across[0, :, at].astype(f32), across[1, :, at].astype(f32)
        rims = beyond[:, at].astype(f32)
        rows_id = iota((length, width), 0)
        first = 3 if start else 0
        tap = [
            jnp.concatenate((taps[t : t + 1, :], taps_over[t : t + 1, :]), axis=1)
            for t in range(first, first + 3)
        ]
        done = []
        for p in range(pieces):
            s, r = p // inner, p % inner
            sub, block = lax.rem(x + r, inner), lax.rem(z + outer - s, outer)
            down, over = (s + 1) % outer, (s + outer - 1) % outer
            back, on = s * inner + (r - 1) % inner, s * inner + (r + 1) % inner
            rim_before = jnp.where(y == 0, rims[down : down + 1], rims[s : s + 1])
            rim_before = jnp.where((block == 0) & (y == 0), 0.0, rim_before)
            rim_after = jnp.where(y == pair - 1, rims[over : over + 1], rims[s : s + 1])
            rim_after = jnp.where((block == outer - 1) & (y == pair - 1), 0.0, rim_after)
            before = jnp.where(sub == 0, rim_before, high[back : back + 1])
            before = jnp.where(c == 0, before, high[p : p + 1])
            after = jnp.where(sub == inner - 1, rim_after, low[on : on + 1])
            after = jnp.where(c == 0, low[p : p + 1], after)
            cells = up[p * length : (p + 1) * length, at].astype(f32)
            left = jnp.where(rows_id == 0, before, pltpu.roll(cells, 1, 0))
            right = jnp.where(rows_id == length - 1, after, pltpu.roll(cells, length - 1, 0))
            done.append(tap[0] * left + tap[1] * cells + tap[2] * right)
        return jnp.concatenate(done, axis=0)

    gate = convolved(width)
    hidden = (convolved(0) * (gate / (1.0 + jnp.exp(-gate)))).astype(bf16)
    for copy in copies:
        copy.wait()
    for half in range(2):
        partial = jnp.dot(hidden, full[half], preferred_element_type=f32).astype(bf16)
        for p in range(pieces):
            outs[half * inner + p % inner][p // inner] = partial[p * length : (p + 1) * length]


def up_projection(rows_in, stacks, pieces):
    outer, rows, cols = stacks[0].shape
    count = sum(r.shape[0] for r in rows_in)
    return pl.pallas_call(
        up_kernel,
        out_shape=(
            jax.ShapeDtypeStruct((count, 4 * cols), bf16),
            jax.ShapeDtypeStruct((2, pieces, 4 * cols), bf16),
            jax.ShapeDtypeStruct((outer, 4 * cols), bf16),
        ),
        in_specs=[pl.BlockSpec(memory_space=pltpu.HBM)] * (8 + len(rows_in)),
        out_specs=tuple(vmem(3)),
        scratch_shapes=[
            pltpu.VMEM((count, rows_in[0].shape[1]), bf16),
            pltpu.VMEM((2, pieces, 4 * cols), f32),
            pltpu.VMEM((2, 2 * outer * rows, 2 * cols), bf16),
            pltpu.SemaphoreType.DMA((4, 2 * outer)),
            pltpu.SemaphoreType.DMA((len(rows_in),)),
        ],
        name="upk",
    )(*stacks, *rows_in)


def down_projection(up, across, beyond, taps, taps_over, held, inner):
    outer = len(held) // 4
    rows, cols = held[0].shape
    length = up.shape[0] // (outer * inner)
    outs = pl.pallas_call(
        functools.partial(down_kernel, outer),
        out_shape=(jax.ShapeDtypeStruct((outer, length, outer * cols), bf16),) * (2 * inner),
        in_specs=vmem(5) + [pl.BlockSpec(memory_space=pltpu.HBM)] * len(held),
        out_specs=tuple(vmem(2 * inner)),
        scratch_shapes=[
            pltpu.VMEM((2, 2 * rows, outer * cols), bf16),
            pltpu.SemaphoreType.DMA((len(held),)),
        ],
        name="downk",
    )(up, across, beyond, taps, taps_over, *held)
    return outs[:inner], outs[inner:]


def edges_of(ends, rim):
    across = lax.ppermute(ends, "tp", ring("tp", pair, 0, 1))
    sizes = (lax.axis_size("sp"), lax.axis_size("tp"))
    hops = [
        (i * sizes[1] + j, (i ^ 1) * sizes[1] + (j ^ 1))
        for i in range(sizes[0])
        for j in range(sizes[1])
    ]
    return across, lax.ppermute(rim, ("sp", "tp"), hops)


def spread_body(
    mixer_input,
    time_step,
    damping,
    input_map,
    readout,
    skip_gain,
    out_gain,
    out_weight,
    residual,
    channel_gain,
    value_weight,
    gate_weight,
    value_taps,
    gate_taps,
    down_weight,
):
    tp_count, sp_count = lax.axis_size("tp"), lax.axis_size("sp")
    outer, inner = sp_count // pair, tp_count // pair
    tok_rows, local_width = mixer_input.shape
    own_rows = tok_rows // tp_count
    model = residual.shape[1]
    z, tp = lax.axis_index("sp") // pair, lax.axis_index("tp")

    value_pieces, gate_pieces, down_pieces = cut_weights(
        (value_weight, gate_weight, down_weight), outer
    )
    value_stacks = spread(value_pieces)
    scal, xt, yt, rows_a, ends = mixer_local(mixer_input, time_step, damping, input_map, readout)
    every = lax.all_to_all(ends, "sp", 0, 0, tiled=True)
    gate_stacks = spread(gate_pieces)
    taps = jnp.concatenate((value_taps, gate_taps))
    taps = lax.dynamic_index_in_dim(taps.reshape(taps.shape[0], outer, -1), z, 1, False)
    taps_over = lax.ppermute(taps, "tp", ring("tp", pair, 0, 1))

    mixed = mixer_carried(scal, xt, yt, rows_a, every, readout, skip_gain, out_gain)
    mixed = lax.all_gather(mixed, "tp", axis=0)
    squares = jnp.sum(mixed[:, local_width:].astype(f32), axis=(0, 1))
    inverse = lax.rsqrt(squares / (local_width * tp_count) + norm_eps)
    channels = mixed[:, :local_width].reshape(local_width * tp_count, tok_rows)
    mixed_rows = lax.dot_general(
        channels, out_weight, (((0,), (0,)), ((), ())), preferred_element_type=f32
    )
    mixed_rows = mixed_rows * inverse[:, None]
    picked = lax.dynamic_slice_in_dim(mixed_rows, tp * own_rows, own_rows, axis=0)
    hidden_state = (residual.astype(f32) + picked).astype(bf16)
    state_wide = hidden_state.astype(f32)
    scale_rows = lax.rsqrt(jnp.mean(state_wide * state_wide, axis=1, keepdims=True) + norm_eps)
    normed = (state_wide * scale_rows * channel_gain[None, :]).astype(bf16)
    rows_in = []
    for s in range(outer):
        got = normed
        if s:
            got = lax.ppermute(normed, "sp", ring("sp", pair, s))
        rows_in += [got] + outer_send(lambda s: got, "tp", pair)[::-1]
    up, ends, rim = up_projection(rows_in, value_stacks + gate_stacks, outer * inner)
    down_stacks = spread_pieces(down_pieces)
    across, beyond = edges_of(ends, rim)
    halves = down_projection(up, across, beyond, taps, taps_over, down_stacks, inner)
    sums = []
    for parts in halves:
        arrived = outer_send(lambda s: parts[s], "tp", pair)
        total = parts[0].astype(f32)
        for got in arrived:
            total = total + got.astype(f32)
        total = total.astype(bf16)
        arrived = outer_send(lambda s: total[outer - s], "sp", pair)
        summed = total[0].astype(f32)
        for got in arrived:
            summed = summed + got.astype(f32)
        sums.append(summed)
    block = down_weight.shape[1]
    summed = jnp.stack([part.reshape(own_rows, outer, block) for part in sums], axis=2)
    return (state_wide + summed.reshape(own_rows, model)).astype(bf16)


def solution(mesh):
    in_specs = (
        P("sp", "tp"),
        P(None, "tp"),
        P(None, "sp", "tp"),
        P(None, None, "tp", None, None),
        P(None, None, "tp", None, None),
        P("tp"),
        P("tp"),
        P(),
        P(("sp", "tp"), None),
        P(),
        P("sp", "tp"),
        P("sp", "tp"),
        P(None, "tp"),
        P(None, "tp"),
        P("tp", "sp"),
    )
    out_specs = P(("sp", "tp"), None)

    def body(*args):
        value_weight = args[10]
        sp, tp = mesh.shape["sp"], mesh.shape["tp"]
        even = sp % pair == 0 and tp % pair == 0
        whole_lanes = even and (value_weight.shape[1] // (sp // pair)) % 128 == 0
        if not whole_lanes:
            return gathered_body(*args)
        return spread_body(*args)

    return jax.shard_map(body, mesh=mesh, in_specs=in_specs, out_specs=out_specs, check_vma=False)
```

```python
import functools
import math

import jax
import jax.numpy as jnp
from jax import lax
from jax.experimental import pallas as pl
from jax.experimental.pallas import tpu as pltpu
from jax.sharding import PartitionSpec as P


norm_eps = 1e-06
f32 = jnp.float32
bf16 = jnp.bfloat16


def split2(a):
    top = a.astype(bf16)
    return top, (a - top.astype(f32)).astype(bf16)


def dot3(a, b):
    rows = a.shape[0]
    a0, a1 = split2(a)
    b0, b1 = split2(b)
    both = jnp.dot(jnp.concatenate((a0, a1), axis=0), b0, preferred_element_type=f32)
    return both[:rows] + both[rows:] + jnp.dot(a0, b1, preferred_element_type=f32)


def four_wide(ref, g):
    return jnp.concatenate([ref[k, p, g] for k in range(2) for p in range(2)], axis=1)


def signed_wide(readout, g):
    parts = [readout[k, p, g] for k in range(2) for p in range(2)]
    return jnp.concatenate((parts[0], -parts[1], parts[2], -parts[3]), axis=1)


def over_rows(a, b):
    return lax.dot_general(a, b, (((0,), (0,)), ((), ())), preferred_element_type=f32)


def cos_sin(coarse, fine, count):
    first = coarse * count
    first = first - jnp.floor(first + 0.5)
    turn = first + fine * count
    half = jnp.floor(2.0 * turn + 0.5)
    angle = (2.0 * math.pi) * (turn - 0.5 * half)
    odd = half - 2.0 * jnp.floor(0.5 * half)
    sign = 1.0 - 2.0 * odd
    z = angle * angle
    sine = jnp.full_like(z, -1.0 / 39916800.0)
    for c in (1.0 / 362880.0, -1.0 / 5040.0, 1.0 / 120.0, -1.0 / 6.0, 1.0):
        sine = sine * z + c
    cosine = jnp.full_like(z, 1.0 / 479001600.0)
    for c in (-1.0 / 3628800.0, 1.0 / 40320.0, -1.0 / 720.0, 1.0 / 24.0, -0.5, 1.0):
        cosine = cosine * z + c
    return cosine * sign, sine * (angle * sign)


def iota(shape, dim):
    return lax.broadcasted_iota(jnp.int32, shape, dim)


def turns_of(states, rows, backward):
    when = iota((states, rows), 1)
    when = rows - 1 - when if backward else when
    return (iota((states, rows), 0) * when).astype(f32)


def local_kernel(scal, x_in, damp, in_map, readout, yt, xt, ends, rows_a):
    groups, rows = damp.shape[1], damp.shape[2]
    chans, states = in_map.shape[3], in_map.shape[4]
    part, quarter = states // 2, 2 * groups
    lane = iota((part, ends.shape[2]), 1)
    slim = iota((8, ends.shape[2]), 1)
    row_id, col_id = iota((rows, rows), 0), iota((rows, rows), 1)
    kept = (row_id <= col_id, row_id >= col_id)
    for k in range(2):
        ones = kept[k].astype(f32).astype(bf16)
        left = damp[k]
        sums = jnp.zeros(left.shape, f32)
        for _ in range(3):
            part_of = left.astype(bf16)
            sums += jnp.dot(part_of, ones, preferred_element_type=f32)
            left = left - part_of.astype(f32)
        rows_a[k] = sums
    xt[...] = x_in[...].astype(f32).T.astype(bf16)
    since = iota((1, rows), 1).astype(f32) + 1.0
    elapsed = (since, rows + 1.0 - since)
    counts = [turns_of(states, rows, k == 1) for k in range(2)]

    def group(g, carry):
        held, spans = carry
        at = pl.ds(pl.multiple_of(g * chans, chans), chans)
        x = xt[at, :]
        drives = over_rows(four_wide(in_map, g), x)
        joined = []
        for k in range(2):
            cosine, sine = cos_sin(scal[0, k, g], scal[1, k, g], counts[k])
            scale = scal[2, k, g]
            drive_r = drives[2 * k * states : (2 * k + 1) * states] * scale
            drive_i = drives[(2 * k + 1) * states : (2 * k + 2) * states] * scale
            turned = jnp.concatenate(
                (cosine * drive_r + sine * drive_i, cosine * drive_i - sine * drive_r), axis=0
            )
            summed = rows_a[k, pl.ds(g, 1), :] + (scal[0, k, g] + scal[1, k, g]) * elapsed[k]
            rows_a[k, pl.ds(g, 1), :] = summed
            across = jnp.broadcast_to(summed, (rows, rows))
            decay = jnp.exp(jnp.where(kept[k], across.T - across, -1e30))
            z = dot3(turned, decay)
            z_r, z_i = z[:states], z[states:]
            s_r = cosine * z_r - sine * z_i
            s_i = cosine * z_i + sine * z_r
            joined += [s_r, s_i]
            last = 0 if k else rows - 1
            spans = jnp.where(slim == k * groups + g, across[:8, last : last + 1], spans)
            for p, s in enumerate((s_r, s_i)):
                col = s[:, last : last + 1]
                for half in range(2):
                    spot = (half * 2 + p) * quarter + k * groups + g
                    held = jnp.where(lane == spot, col[half * part : (half + 1) * part], held)
        yt[at, :] = dot3(signed_wide(readout, g), jnp.concatenate(joined, axis=0))
        return held, spans

    start = (jnp.zeros(lane.shape, f32), jnp.zeros(slim.shape, f32))
    held, spans = lax.fori_loop(0, groups, group, start, unroll=4)
    for peer in range(ends.shape[0]):
        ends[peer, :part] = held
        ends[peer, part:] = spans


def carry_kernel(scal, xt, rows_a, every, readout, yt, skip, gain, out, wide):
    groups, rows = rows_a.shape[1], rows_a.shape[2]
    chans, states = readout.shape[3], readout.shape[4]
    blocks = every.shape[0]
    part, quarter = states // 2, 2 * groups
    mine = lax.axis_index("sp")
    number = iota((states, quarter), 0).astype(f32)
    backward = iota((states, quarter), 1) >= groups
    spot = iota((1, quarter), 1)
    coarse = jnp.zeros((1, quarter), f32)
    fine = jnp.zeros((1, quarter), f32)
    for k in range(2):
        for g in range(groups):
            coarse = jnp.where(spot == k * groups + g, scal[0, k, g], coarse)
            fine = jnp.where(spot == k * groups + g, scal[1, k, g], fine)
    width = skip.shape[1]
    wide[0] = jnp.broadcast_to(skip[...], (rows, width)).T
    wide[1] = jnp.broadcast_to(gain[...], (rows, width)).T
    far_r, far_i = cos_sin(coarse, fine, number * rows)
    near_r, near_i = cos_sin(coarse, fine, number)

    def piece(b, p):
        ref = every.at[b]
        return jnp.concatenate(
            [ref[:part, (h * 2 + p) * quarter : (h * 2 + p + 1) * quarter] for h in range(2)], axis=0
        )

    c_r = jnp.zeros((states, quarter), f32)
    c_i = jnp.zeros((states, quarter), f32)
    for b in range(blocks - 1):
        other = blocks - 1 - b
        e_r = jnp.where(backward, piece(other, 0), piece(b, 0))
        e_i = jnp.where(backward, piece(other, 1), piece(b, 1))
        span = jnp.where(
            backward[:1], every[other, part : part + 1, :quarter], every[b, part : part + 1, :quarter]
        )
        fade = jnp.exp(-span)
        n_r = fade * (far_r * c_r - far_i * c_i) + e_r
        n_i = fade * (far_r * c_i + far_i * c_r) + e_i
        place_in = jnp.where(backward, blocks - 1 - mine, mine)
        c_r = jnp.where(b < place_in, n_r, c_r)
        c_i = jnp.where(b < place_in, n_i, c_i)
    w_r = near_r * c_r - near_i * c_i
    w_i = near_r * c_i + near_i * c_r
    counts = [turns_of(states, rows, k == 1) for k in range(2)]
    squares = jnp.zeros((8, rows), f32)
    for g in range(groups):
        at = pl.ds(g * chans, chans)
        total = yt[at, :] + wide[0, at, :] * xt[at, :].astype(f32)
        joined = []
        for k in range(2):
            cosine, sine = cos_sin(scal[0, k, g], scal[1, k, g], counts[k])
            l = k * groups + g
            a, b = w_r[:, l : l + 1], w_i[:, l : l + 1]
            fade = jnp.exp(-rows_a[k, g : g + 1, :])
            joined += [(cosine * a - sine * b) * fade, (cosine * b + sine * a) * fade]
        total += dot3(signed_wide(readout, g), jnp.concatenate(joined, axis=0))
        for r in range(0, chans, 8):
            squares += total[r : r + 8] * total[r : r + 8]
        out[at, :] = (total * wide[1, at, :]).astype(bf16)
    square = jnp.sum(squares, axis=0, keepdims=True)
    top = square.astype(bf16)
    rest = square - top.astype(f32)
    mid = rest.astype(bf16)
    low = (rest - mid.astype(f32)).astype(bf16)
    extra = out.shape[0] - groups * chans
    which = iota((extra, rows), 0)
    tail = jnp.where(which == 0, top.astype(f32), jnp.where(which == 1, mid.astype(f32), low.astype(f32)))
    tail = jnp.where(which < 3, tail, 0.0)
    out[pl.ds(groups * chans, extra), :] = tail.astype(bf16)


square_rows = 16


def vmem(count):
    return [pl.BlockSpec(memory_space=pltpu.VMEM)] * count


def mixer_local(mixer_input, time_step, damping, input_map, readout):
    rows, width = mixer_input.shape
    groups = time_step.shape[1]
    states = input_map.shape[3]
    half_step = 0.5 * time_step
    coarse = jnp.floor(half_step * 2048.0) / 2048.0
    scal = jnp.stack((coarse, half_step - coarse, jnp.sqrt(-jnp.expm1(-time_step))))
    damp = jnp.swapaxes(damping, 1, 2)
    lanes = 8 * groups
    smem = pl.BlockSpec(memory_space=pltpu.SMEM)
    yt, xt, ends, rows_a = pl.pallas_call(
        local_kernel,
        out_shape=(
            jax.ShapeDtypeStruct((width, rows), f32),
            jax.ShapeDtypeStruct((width, rows), bf16),
            jax.ShapeDtypeStruct((lax.axis_size("sp"), states // 2 + 8, lanes), f32),
            jax.ShapeDtypeStruct(damp.shape, f32),
        ),
        in_specs=[smem] + vmem(4),
        out_specs=tuple(vmem(4)),
        name="mixl",
    )(scal, mixer_input, damp, jnp.swapaxes(input_map, 3, 4), readout)
    return scal, xt, yt, rows_a, ends


def mixer_carried(scal, xt, yt, rows_a, every, readout, skip_gain, out_gain):
    width, rows = xt.shape
    smem = pl.BlockSpec(memory_space=pltpu.SMEM)
    return pl.pallas_call(
        carry_kernel,
        out_shape=jax.ShapeDtypeStruct((width + square_rows, rows), bf16),
        in_specs=[smem] + vmem(7),
        out_specs=pl.BlockSpec(memory_space=pltpu.VMEM),
        scratch_shapes=[pltpu.VMEM((2, width, rows), f32)],
        name="mixc",
    )(scal, xt, rows_a, every, readout, yt, skip_gain[None, :], out_gain[None, :])


def with_halo(cells, axis):
    count = lax.axis_size(axis)
    return jnp.concatenate(
        [
            lax.ppermute(cells[-1:], axis, [(i, i + 1) for i in range(count - 1)]),
            cells,
            lax.ppermute(cells[:1], axis, [(i + 1, i) for i in range(count - 1)]),
        ],
        axis=0,
    )


def gathered_body(
    mixer_input,
    time_step,
    damping,
    input_map,
    readout,
    skip_gain,
    out_gain,
    out_weight,
    residual,
    channel_gain,
    value_weight,
    gate_weight,
    value_taps,
    gate_taps,
    down_weight,
):
    tp_count = lax.axis_size("tp")
    tok_rows, local_width = mixer_input.shape
    residual_rows = lax.all_gather(residual, "tp", axis=0, tiled=True)
    scal, xt, yt, rows_a, ends = mixer_local(mixer_input, time_step, damping, input_map, readout)
    every = lax.all_to_all(ends, "sp", 0, 0, tiled=True)
    mixed = mixer_carried(scal, xt, yt, rows_a, every, readout, skip_gain, out_gain)
    mixed = lax.all_gather(mixed, "tp", axis=0)
    squares = jnp.sum(mixed[:, local_width:].astype(f32), axis=(0, 1))
    inverse = lax.rsqrt(squares / (local_width * tp_count) + norm_eps)
    channels = mixed[:, :local_width].reshape(local_width * tp_count, tok_rows)
    mixed_rows = (
        lax.dot_general(channels, out_weight, (((0,), (0,)), ((), ())), preferred_element_type=f32)
        * inverse[:, None]
    )
    hidden_state = (residual_rows.astype(f32) + mixed_rows).astype(bf16)
    state_wide = hidden_state.astype(f32)
    scale_rows = lax.rsqrt(jnp.mean(state_wide * state_wide, axis=1, keepdims=True) + norm_eps)
    block_rows = (state_wide * scale_rows * channel_gain[None, :]).astype(bf16)
    hidden_width = value_weight.shape[1]
    value_up = jnp.dot(
        block_rows,
        lax.all_gather(value_weight, "sp", axis=0, tiled=True),
        preferred_element_type=f32,
    )
    gate_up = jnp.dot(
        block_rows,
        lax.all_gather(gate_weight, "sp", axis=0, tiled=True),
        preferred_element_type=f32,
    )
    both_up = jnp.concatenate((value_up.astype(bf16), gate_up.astype(bf16)), axis=1)
    padded = with_halo(both_up, "sp")
    taps = jnp.concatenate((value_taps, gate_taps), axis=1)
    convolved = (
        taps[0] * padded[:-2].astype(f32)
        + taps[1] * padded[1:-1].astype(f32)
        + taps[2] * padded[2:].astype(f32)
    )
    hidden = (convolved[:, :hidden_width] * jax.nn.silu(convolved[:, hidden_width:])).astype(bf16)
    down_full = lax.all_gather(down_weight, "sp", axis=1, tiled=True)
    partial = jnp.dot(hidden, down_full, preferred_element_type=f32).astype(bf16)
    pieces = lax.all_to_all(
        partial.reshape(tp_count, tok_rows // tp_count, -1), "tp", 0, 0, tiled=True
    )
    mine = lax.axis_index("tp") * (tok_rows // tp_count)
    own = lax.dynamic_slice_in_dim(state_wide, mine, tok_rows // tp_count, axis=0)
    return (own + jnp.sum(pieces.astype(f32), axis=0)).astype(bf16)


def ring(axis, inner, step, low=0):
    size = lax.axis_size(axis)
    outer = size // inner
    return [
        (i, ((i // inner + step) % outer) * inner + (i + low) % inner) for i in range(size)
    ]


def outer_send(pick, axis, inner):
    outer = lax.axis_size(axis) // inner
    return [lax.ppermute(pick(s), axis, ring(axis, inner, s)) for s in range(1, outer)]


def cut_weights(weights, outer):
    def shape_of(weight):
        rows, cols = weight.shape
        return (rows // outer, cols) if rows > cols else (rows, cols // outer)

    def kernel(*refs):
        ins, outs, sems = refs[: len(weights)], refs[len(weights) : -1], refs[-1]
        mine = lax.axis_index("sp") // pair
        copies = []
        for w, ref in enumerate(ins):
            for s in range(outer):
                there = lax.rem(mine + s, outer)
                out = outs[w * outer + s]
                rows, cols = out.shape
                if rows == ref.shape[0]:
                    part = ref.at[:, pl.ds(pl.multiple_of(there * cols, cols), cols)]
                else:
                    part = ref.at[pl.ds(pl.multiple_of(there * rows, rows), rows), :]
                copy = pltpu.make_async_copy(part, out, sems.at[w, s])
                copy.start()
                copies.append(copy)
        for copy in copies:
            copy.wait()

    outs = tuple(
        jax.ShapeDtypeStruct(shape_of(weight), bf16) for weight in weights for _ in range(outer)
    )
    pieces = pl.pallas_call(
        kernel,
        out_shape=outs,
        in_specs=[pl.BlockSpec(memory_space=pltpu.HBM)] * len(weights),
        out_specs=tuple(vmem(len(outs))),
        scratch_shapes=[pltpu.SemaphoreType.DMA((len(weights), outer))],
        name="cutk",
    )(*weights)
    return [pieces[w * outer : (w + 1) * outer] for w in range(len(weights))]


def spread_pieces(pieces):
    outer = len(pieces)
    own = [pieces[0]]
    for s in range(1, outer):
        own.append(lax.ppermute(pieces[s], "sp", ring("sp", pair, s)))
    beside = []
    for s in range(outer):
        beside.append(lax.ppermute(own[s], "sp", ring("sp", pair, 0, 1)))
    over = ring("tp", pair, 0, 1)
    across = []
    for piece in own + beside:
        across.append(lax.ppermute(piece, "tp", over))
    return own + beside + across


def spread(pieces):
    moved = outer_send(lambda s: pieces[s], "sp", pair)
    own = jnp.stack([pieces[0]] + moved)
    beside = lax.ppermute(own, "sp", ring("sp", pair, 0, 1))
    over = ring("tp", pair, 0, 1)
    across = lax.ppermute(own, "tp", over)
    return own, beside, across, lax.ppermute(beside, "tp", over)


pair = 2


def row_block(outer, which, step):
    sp = lax.axis_index("sp")
    far = lax.rem(sp // pair + outer - step, outer)
    return far * pair + lax.rem(sp + which, pair)


def up_kernel(*refs):
    stacks, (out, edges, rim, x, last, full, sems, row_sems) = refs[:8], refs[-8:]
    rows_in = refs[8:-8]
    outer, rows, cols = stacks[0].shape
    at, row_copies = 0, []
    for n, ref in enumerate(rows_in):
        size = ref.shape[0]
        copy = pltpu.make_async_copy(ref, x.at[at : at + size, :], row_sems.at[n])
        copy.start()
        row_copies.append(copy)
        at += size
    groups = []
    for kind in range(2):
        copies = []
        for core in range(2):
            for which in range(2):
                ref = stacks[kind * 4 + core * 2 + which]
                for s in range(outer):
                    first = pl.multiple_of(row_block(outer, which, s) * rows, rows)
                    copy = pltpu.make_async_copy(
                        ref.at[s],
                        full.at[kind, pl.ds(first, rows), pl.ds(core * cols, cols)],
                        sems.at[kind * 2 + core, which * outer + s],
                    )
                    copy.start()
                    copies.append(copy)
        groups.append(copies)
    for copy in row_copies:
        copy.wait()
    pieces = edges.shape[1]
    for kind, copies in enumerate(groups):
        for copy in copies:
            copy.wait()
        part = jnp.dot(x[...], full[kind], preferred_element_type=f32)
        first = 2 * kind * cols
        out[:, first : first + 2 * cols] = part.astype(bf16)
        length = part.shape[0] // pieces
        for p in range(pieces):
            for end, at in ((0, p * length), (1, (p + 1) * length - 1)):
                row = part[at : at + 1]
                last[end, p : p + 1, first : first + cols] = row[:, cols:]
                last[end, p : p + 1, first + cols : first + 2 * cols] = row[:, :cols]
    edges[...] = last[...].astype(bf16)
    tp = lax.axis_index("tp")
    x_at, c_at = tp // pair, lax.rem(tp, pair)
    inner = pieces // outer
    for s in range(outer):
        row = jnp.zeros((1, last.shape[2]), f32)
        for r in range(inner):
            sub = lax.rem(x_at + r, inner)
            low = last[0, s * inner + r : s * inner + r + 1, :]
            high = last[1, s * inner + r : s * inner + r + 1, :]
            row = jnp.where((c_at == 0) & (sub == 0), low, row)
            row = jnp.where((c_at == 1) & (sub == inner - 1), high, row)
        last[0, s : s + 1, :] = row
    rim[...] = last[0, :outer, :].astype(bf16)


def load_down(held, outer, full, sems):
    rows, cols = held[0].shape
    y = lax.rem(lax.axis_index("sp"), pair)
    copies = []
    for core in range(2):
        for s in range(outer):
            far = lax.rem(lax.axis_index("sp") // pair + outer - s, outer)
            first = pl.multiple_of(far * cols, cols)
            for which in range(2):
                n = (core * 2 + which) * outer + s
                into = lax.rem(y + which, pair)
                copy = pltpu.make_async_copy(
                    held[n],
                    full.at[into, pl.ds(core * rows, rows), pl.ds(first, cols)],
                    sems.at[n],
                )
                copy.start()
                copies.append(copy)
    return copies


def down_kernel(outer, up, across, beyond, taps, taps_over, *refs):
    held, outs, (full, sems) = refs[: 4 * outer], refs[4 * outer : -2], refs[-2:]
    copies = load_down(held, outer, full, sems)
    rows = held[0].shape[0]
    width = 2 * rows
    count, pieces = up.shape[0], across.shape[1]
    length, inner = count // pieces, pieces // outer
    sp, tp = lax.axis_index("sp"), lax.axis_index("tp")
    z, y, x, c = sp // pair, lax.rem(sp, pair), tp // pair, lax.rem(tp, pair)

    def convolved(start):
        at = slice(start, start + width)
        low, high = across[0, :, at].astype(f32), across[1, :, at].astype(f32)
        rims = beyond[:, at].astype(f32)
        rows_id = iota((length, width), 0)
        first = 3 if start else 0
        tap = [
            jnp.concatenate((taps[t : t + 1, :], taps_over[t : t + 1, :]), axis=1)
            for t in range(first, first + 3)
        ]
        done = []
        for p in range(pieces):
            s, r = p // inner, p % inner
            sub, block = lax.rem(x + r, inner), lax.rem(z + outer - s, outer)
            down, over = (s + 1) % outer, (s + outer - 1) % outer
            back, on = s * inner + (r - 1) % inner, s * inner + (r + 1) % inner
            rim_before = jnp.where(y == 0, rims[down : down + 1], rims[s : s + 1])
            rim_before = jnp.where((block == 0) & (y == 0), 0.0, rim_before)
            rim_after = jnp.where(y == pair - 1, rims[over : over + 1], rims[s : s + 1])
            rim_after = jnp.where((block == outer - 1) & (y == pair - 1), 0.0, rim_after)
            before = jnp.where(sub == 0, rim_before, high[back : back + 1])
            before = jnp.where(c == 0, before, high[p : p + 1])
            after = jnp.where(sub == inner - 1, rim_after, low[on : on + 1])
            after = jnp.where(c == 0, low[p : p + 1], after)
            cells = up[p * length : (p + 1) * length, at].astype(f32)
            left = jnp.where(rows_id == 0, before, pltpu.roll(cells, 1, 0))
            right = jnp.where(rows_id == length - 1, after, pltpu.roll(cells, length - 1, 0))
            done.append(tap[0] * left + tap[1] * cells + tap[2] * right)
        return jnp.concatenate(done, axis=0)

    gate = convolved(width)
    hidden = (convolved(0) * (gate / (1.0 + jnp.exp(-gate)))).astype(bf16)
    for copy in copies:
        copy.wait()
    for half in range(2):
        partial = jnp.dot(hidden, full[half], preferred_element_type=f32).astype(bf16)
        for p in range(pieces):
            outs[half * inner + p % inner][p // inner] = partial[p * length : (p + 1) * length]


def up_projection(rows_in, stacks, pieces):
    outer, rows, cols = stacks[0].shape
    count = sum(r.shape[0] for r in rows_in)
    return pl.pallas_call(
        up_kernel,
        out_shape=(
            jax.ShapeDtypeStruct((count, 4 * cols), bf16),
            jax.ShapeDtypeStruct((2, pieces, 4 * cols), bf16),
            jax.ShapeDtypeStruct((outer, 4 * cols), bf16),
        ),
        in_specs=[pl.BlockSpec(memory_space=pltpu.HBM)] * (8 + len(rows_in)),
        out_specs=tuple(vmem(3)),
        scratch_shapes=[
            pltpu.VMEM((count, rows_in[0].shape[1]), bf16),
            pltpu.VMEM((2, pieces, 4 * cols), f32),
            pltpu.VMEM((2, 2 * outer * rows, 2 * cols), bf16),
            pltpu.SemaphoreType.DMA((4, 2 * outer)),
            pltpu.SemaphoreType.DMA((len(rows_in),)),
        ],
        name="upk",
    )(*stacks, *rows_in)


def down_projection(up, across, beyond, taps, taps_over, held, inner):
    outer = len(held) // 4
    rows, cols = held[0].shape
    length = up.shape[0] // (outer * inner)
    outs = pl.pallas_call(
        functools.partial(down_kernel, outer),
        out_shape=(jax.ShapeDtypeStruct((outer, length, outer * cols), bf16),) * (2 * inner),
        in_specs=vmem(5) + [pl.BlockSpec(memory_space=pltpu.HBM)] * len(held),
        out_specs=tuple(vmem(2 * inner)),
        scratch_shapes=[
            pltpu.VMEM((2, 2 * rows, outer * cols), bf16),
            pltpu.SemaphoreType.DMA((len(held),)),
        ],
        name="downk",
    )(up, across, beyond, taps, taps_over, *held)
    return outs[:inner], outs[inner:]


def edges_of(ends, rim):
    across = lax.ppermute(ends, "tp", ring("tp", pair, 0, 1))
    sizes = (lax.axis_size("sp"), lax.axis_size("tp"))
    hops = [
        (i * sizes[1] + j, (i ^ 1) * sizes[1] + (j ^ 1))
        for i in range(sizes[0])
        for j in range(sizes[1])
    ]
    return across, lax.ppermute(rim, ("sp", "tp"), hops)


def spread_body(
    mixer_input,
    time_step,
    damping,
    input_map,
    readout,
    skip_gain,
    out_gain,
    out_weight,
    residual,
    channel_gain,
    value_weight,
    gate_weight,
    value_taps,
    gate_taps,
    down_weight,
):
    tp_count, sp_count = lax.axis_size("tp"), lax.axis_size("sp")
    outer, inner = sp_count // pair, tp_count // pair
    tok_rows, local_width = mixer_input.shape
    own_rows = tok_rows // tp_count
    model = residual.shape[1]
    z, tp = lax.axis_index("sp") // pair, lax.axis_index("tp")

    value_pieces, gate_pieces, down_pieces = cut_weights(
        (value_weight, gate_weight, down_weight), outer
    )
    value_stacks = spread(value_pieces)
    scal, xt, yt, rows_a, ends = mixer_local(mixer_input, time_step, damping, input_map, readout)
    every = lax.all_to_all(ends, "sp", 0, 0, tiled=True)
    gate_stacks = spread(gate_pieces)
    taps = jnp.concatenate((value_taps, gate_taps))
    taps = lax.dynamic_index_in_dim(taps.reshape(taps.shape[0], outer, -1), z, 1, False)
    taps_over = lax.ppermute(taps, "tp", ring("tp", pair, 0, 1))

    mixed = mixer_carried(scal, xt, yt, rows_a, every, readout, skip_gain, out_gain)
    mixed = lax.all_gather(mixed, "tp", axis=0)
    mixed = lax.dynamic_slice_in_dim(mixed, tp * own_rows, own_rows, axis=2)
    squares = jnp.sum(mixed[:, local_width:].astype(f32), axis=(0, 1))
    inverse = lax.rsqrt(squares / (local_width * tp_count) + norm_eps)
    channels = mixed[:, :local_width].reshape(local_width * tp_count, own_rows)
    mixed_rows = lax.dot_general(
        channels, out_weight, (((0,), (0,)), ((), ())), preferred_element_type=f32
    )
    hidden_state = (residual.astype(f32) + mixed_rows * inverse[:, None]).astype(bf16)
    state_wide = hidden_state.astype(f32)
    scale_rows = lax.rsqrt(jnp.mean(state_wide * state_wide, axis=1, keepdims=True) + norm_eps)
    normed = (state_wide * scale_rows * channel_gain[None, :]).astype(bf16)
    rows_in = []
    for s in range(outer):
        got = normed
        if s:
            got = lax.ppermute(normed, "sp", ring("sp", pair, s))
        rows_in += [got] + outer_send(lambda s: got, "tp", pair)[::-1]
    up, ends, rim = up_projection(rows_in, value_stacks + gate_stacks, outer * inner)
    down_stacks = spread_pieces(down_pieces)
    across, beyond = edges_of(ends, rim)
    halves = down_projection(up, across, beyond, taps, taps_over, down_stacks, inner)
    sums = []
    for parts in halves:
        arrived = outer_send(lambda s: parts[s], "tp", pair)
        total = parts[0].astype(f32)
        for got in arrived:
            total = total + got.astype(f32)
        total = total.astype(bf16)
        arrived = outer_send(lambda s: total[outer - s], "sp", pair)
        summed = total[0].astype(f32)
        for got in arrived:
            summed = summed + got.astype(f32)
        sums.append(summed)
    block = down_weight.shape[1]
    summed = jnp.stack([part.reshape(own_rows, outer, block) for part in sums], axis=2)
    return (state_wide + summed.reshape(own_rows, model)).astype(bf16)


def solution(mesh):
    in_specs = (
        P("sp", "tp"),
        P(None, "tp"),
        P(None, "sp", "tp"),
        P(None, None, "tp", None, None),
        P(None, None, "tp", None, None),
        P("tp"),
        P("tp"),
        P(),
        P(("sp", "tp"), None),
        P(),
        P("sp", "tp"),
        P("sp", "tp"),
        P(None, "tp"),
        P(None, "tp"),
        P("tp", "sp"),
    )
    out_specs = P(("sp", "tp"), None)

    def body(*args):
        value_weight = args[10]
        sp, tp = mesh.shape["sp"], mesh.shape["tp"]
        even = sp % pair == 0 and tp % pair == 0
        whole_lanes = even and (value_weight.shape[1] // (sp // pair)) % 128 == 0
        if not whole_lanes:
            return gathered_body(*args)
        return spread_body(*args)

    return jax.shard_map(body, mesh=mesh, in_specs=in_specs, out_specs=out_specs, check_vma=False)
```
